256 devices in a mesh: grp: 2 (over z), ep: 64 (over y, x), tp: 2 (over core).
Axes of the slice: x: 8, y: 8, z: 2, core: 2. Of those that a mesh axis runs over, the one named last changes fastest.
The devices are a block of a 8x8x16 slice.
Arguments:
- tokens: bfloat16 [65536, 2048], P(('grp', 'ep', 'tp')), parts along dimension 0, may hold values from -6 to 6
- norm_gain: float32 [2048], replicated, may hold values from 0.1 to 1.9
- expert_ids: int32 [65536, 2], P(('grp', 'ep', 'tp')), parts along dimension 0, may hold values from 0 to 127, all different within a row; in each aligned block of 256 rows (0 to 255, 256 to 511, ...) at most 8 rows name the same one
- gate_values: float32 [65536, 2], P(('grp', 'ep', 'tp')), parts along dimension 0, may hold values from 0.2 to 2
- w_gate: bfloat16 [128, 2048, 512], P('ep', None, 'tp'), may hold values from -0.125 to 0.125
- w_up: bfloat16 [128, 2048, 512], P('ep', None, 'tp'), may hold values from -0.125 to 0.125
- w_down: bfloat16 [128, 512, 2048], P('ep', 'tp'), may hold values from -0.25 to 0.25
- s_gate: bfloat16 [2048, 512], P(None, 'tp'), may hold values from -0.125 to 0.125
- s_up: bfloat16 [2048, 512], P(None, 'tp'), may hold values from -0.125 to 0.125
- s_down: bfloat16 [512, 2048], P('tp'), may hold values from -0.25 to 0.25
Outputs:
- mixed: bfloat16 [65536, 2048], P(('grp', 'ep', 'tp')), parts along dimension 0
The draws below stay inside these ranges and needn't reach their ends.
There are 2 independent parts, one for each index of `grp`. The reference program is written for one: setup_inputs(seed, part) draws one part's arguments, and reference() takes and returns one part's arrays. A program takes and returns all parts, laid end to end along the dimension named above; an argument that names none is the same for every part. Nothing has to cross between parts.
Inputs may be any that keep to these rules, and one draw needn't show every extreme that they name: `expert_ids`: each row names 2 different experts. Within the rows of one device no expert is named by more than 8 rows, a bound that some block reaches.
All inputs are finite; a program needn't handle non-finite values.
Results may differ from the reference program's by a relative error of at most 0.0068.
Values may be sent and summed in bfloat16 or wider, within the bound.
A program may use at most 128 MiB of HBM per device.

```python
import math
import jax
import jax.numpy as jnp
import numpy as np
from jax import lax

D = 2048
FF = 512
SFF = 512
TOPK = 2
TOK_DEV = 256
EXPERTS = 128
TOKENS = 32768
CAP = 8
N_EP = 64
N_TP = 2


def steps_of(stream_key, dims, shards, low, top_value):
    def one(dim, shards_of):
        heights = jax.random.uniform(jax.random.fold_in(jax.random.fold_in(stream_key, 6), dim), (shards_of,), jnp.float32, low / len(shards), top_value / len(shards))
        return jnp.repeat(jnp.exp(heights), dims[dim] // shards_of).reshape((-1,) + (1,) * (len(dims) - dim - 1))

    loudness = one(*shards[0])
    for cut in shards[1:]:
        loudness = loudness * one(*cut)
    return loudness


def shared_out(key, own, number, rows, amount, top, bound, lean):
    ranking = jax.random.permutation(key, amount)
    heavy_load, common = portions_of(amount, rows * top, bound, lean, True), portions_of(amount, rows * top, bound, lean, False)
    places = jnp.arange(amount)

    def named(tallies, rotation):
        used = int((tallies > 0).sum())
        fixed = max(1, used // 4)
        moved = fixed + (places - fixed + rotation * (used - fixed)) % max(1, amount - fixed)
        return jnp.zeros((amount,), jnp.int32).at[ranking[jnp.where(places < fixed, places, moved)]].set(jnp.asarray(tallies, jnp.int32))

    tallies = jnp.where(number % 4 == 0, named(heavy_load, number // 4), named(common, number - number // 4 - 1))
    mixed = jax.random.permutation(jax.random.fold_in(own, 3), amount)
    donor, taker = mixed[0:amount // 2 * 2:2], mixed[1:amount // 2 * 2:2]
    slack = jnp.minimum(tallies[donor] - 1, bound - tallies[taker]) // 2
    slack = jnp.where((donor == ranking[0]) | (taker == ranking[0]) | (tallies[taker] == 0), 0, jnp.maximum(slack, 0))
    moved = jax.random.randint(jax.random.fold_in(own, 4), (amount // 2,), 0, 1 << 20) % (slack + 1)
    tallies = tallies.at[donor].add(-moved).at[taker].add(moved)
    items = jnp.searchsorted(jnp.cumsum(tallies), jnp.arange(rows * top), side="right").astype(jnp.int32)
    table = items.reshape(top, rows).T
    table = table[jax.random.permutation(jax.random.fold_in(own, 1), rows)]
    rotation = jax.random.randint(jax.random.fold_in(own, 2), (rows, 1), 0, top)
    return jnp.take_along_axis(table, (jnp.arange(top)[None, :] + rotation) % top, axis=1)


def portions_of(count, total, reach, skew, full):
    weights = [(1 << 20) // math.isqrt(grade ** skew) + 1 for grade in range(1, count + 1)]
    largest = reach if full else min(reach, max(-(-total // count), total * weights[0] // sum(weights)))
    least = 1 if total - largest >= count - 1 else 0
    given, rest = [largest] + [least] * (count - 1), total - largest - least * (count - 1)
    while rest > 0:
        free = [i for i in range(1, count) if given[i] < largest] or [i for i in range(1, count) if given[i] < reach]
        mass, remaining = sum([weights[i] for i in free]), rest
        for i in free:
            more = min(reach - given[i], max(1, remaining * weights[i] // mass), rest)
            given[i] = given[i] + more
            rest = rest - more
    return np.array(given)


def normal_values(key, shape, spread, most, shards=(), kind=jnp.bfloat16):
    entries = spread * jax.random.normal(key, shape, jnp.float32)
    if shards:
        entries = entries * steps_of(key, shape, shards, -0.22, 0.18)
    return jnp.clip(entries, -most, most).astype(kind)


def setup_inputs(seed: int = 0, part: int = 0) -> dict:
    key_of = jax.random.split(jax.random.key(seed), 11)
    part_keys = jax.random.split(jax.random.fold_in(key_of[10], part), 11)
    tokens = normal_values(part_keys[0], (TOKENS, D), 1.0, 6.0, ((0, 128),))
    norm_gain = jnp.clip(1.0 + 0.18 * jax.random.normal(key_of[1], (D,), jnp.float32), 0.1, 1.9)
    expert_ids_keys = jax.random.split(jax.random.fold_in(part_keys[2], 1), TOKENS // TOK_DEV)
    expert_ids_turns = jax.random.permutation(jax.random.fold_in(part_keys[2], 3), TOKENS // TOK_DEV)
    expert_ids = jax.vmap(lambda own, number: shared_out(jax.random.fold_in(part_keys[2], 2), own, number, TOK_DEV, EXPERTS, TOPK, CAP, 2))(expert_ids_keys, expert_ids_turns).reshape((TOKENS, TOPK))
    gate_values = jnp.clip(jnp.exp(math.log(2.0) - 2.3025851 * jax.random.uniform(part_keys[3], (TOKENS, TOPK), jnp.float32) ** steps_of(part_keys[3], (TOKENS, TOPK), ((0, 128),), -0.2, 0.2)), 0.2, 2.0)
    w_gate = normal_values(key_of[4], (EXPERTS, D, FF), D ** -0.5, 0.125, ((0, 64), (2, 2)))
    w_up = normal_values(key_of[5], (EXPERTS, D, FF), D ** -0.5, 0.125, ((0, 64), (2, 2)))
    w_down = normal_values(key_of[6], (EXPERTS, FF, D), FF ** -0.5, 0.25, ((0, 64), (1, 2)))
    s_gate = normal_values(key_of[7], (D, SFF), D ** -0.5, 0.125, ((1, 2),))
    s_up = normal_values(key_of[8], (D, SFF), D ** -0.5, 0.125, ((1, 2),))
    s_down = normal_values(key_of[9], (SFF, D), SFF ** -0.5, 0.25, ((0, 2),))
    return dict(tokens=tokens, norm_gain=norm_gain, expert_ids=expert_ids, gate_values=gate_values, w_gate=w_gate, w_up=w_up, w_down=w_down, s_gate=s_gate, s_up=s_up, s_down=s_down)


def reference(tokens, norm_gain, expert_ids, gate_values, w_gate, w_up, w_down, s_gate, s_up, s_down):
    n_tok = tokens.shape[0]
    width = tokens.shape[1]
    topk = expert_ids.shape[1]
    experts_n = w_gate.shape[0]
    xf = tokens.astype(jnp.float32)
    scale = lax.rsqrt(lax.optimization_barrier(jnp.mean(xf * xf, axis=-1, keepdims=True)) + 1e-06)
    normed = (xf * scale * norm_gain.astype(jnp.float32)).astype(jnp.bfloat16)
    s_first = jnp.dot(normed, s_gate, preferred_element_type=jnp.float32)
    s_second = jnp.dot(normed, s_up, preferred_element_type=jnp.float32)
    s_hidden = (jax.nn.silu(s_first) * s_second).astype(jnp.bfloat16)
    shared = jnp.dot(s_hidden, s_down, preferred_element_type=jnp.float32)
    flat_e = expert_ids.reshape(-1).astype(jnp.int32)
    total = flat_e.shape[0]
    order = jnp.argsort(flat_e, stable=True).astype(jnp.int32)
    counts = jnp.bincount(flat_e, length=experts_n).astype(jnp.int32)
    starts = (jnp.cumsum(counts) - counts).astype(jnp.int32)
    most = N_EP * N_TP * CAP
    sorted_tok = jnp.concatenate([(order // topk).astype(jnp.int32), jnp.full((most,), n_tok, jnp.int32)])
    padded = jnp.concatenate([normed, jnp.zeros((1, width), jnp.bfloat16)], axis=0)

    def one_expert(expert):
        index = lax.dynamic_slice(sorted_tok, (starts[expert].astype(jnp.int32),), (most,))
        valid = jnp.arange(most, dtype=jnp.int32) < counts[expert]
        index = jnp.where(valid, index, n_tok).astype(jnp.int32)
        rows = padded[index]
        first = jnp.dot(rows, w_gate[expert], preferred_element_type=jnp.float32)
        second = jnp.dot(rows, w_up[expert], preferred_element_type=jnp.float32)
        hidden = (jax.nn.silu(first) * second).astype(jnp.bfloat16)
        return jnp.dot(hidden, w_down[expert], preferred_element_type=jnp.float32).astype(jnp.bfloat16)
    results = lax.map(one_expert, jnp.arange(experts_n, dtype=jnp.int32))
    inverse = jnp.zeros((total,), jnp.int32).at[order].set(jnp.arange(total, dtype=jnp.int32))
    rank = (inverse - starts[flat_e]).astype(jnp.int32)
    picked = results[flat_e, rank].reshape(n_tok, topk, width)
    routed = lax.optimization_barrier(jnp.sum(gate_values.astype(jnp.float32)[:, :, None] * picked.astype(jnp.float32), axis=1))
    return (shared + routed).astype(jnp.bfloat16)
```

```python
import functools
import math

import jax
import jax.numpy as jnp
from jax import lax
from jax.experimental import pallas as pl
from jax.experimental.pallas import tpu as pltpu
from jax.sharding import PartitionSpec as P

MESH = pl.DeviceIdType.MESH
BF16, F32 = jnp.bfloat16, jnp.float32


def silu_mul(first, second):
    return first * (1.0 / (1.0 + jnp.exp(-first))) * second


def kernel(
    n_ep,
    topk,
    cap,
    tokens,
    gain,
    ids,
    ids_t,
    gates,
    w_gate,
    w_up,
    w_down,
    s_gate,
    s_up,
    s_down,
    out,
    normed,
    sent,
    arrived,
    results,
    returned,
    hidden,
    total,
    wg,
    wu,
    wd,
    sg,
    su,
    sd,
    local_sem,
    w_send,
    w_recv,
    go_send,
    go_recv,
    back_send,
    back_recv,
):
    n_rows, width = tokens.shape
    local_exp = w_gate.shape[0]
    half = w_gate.shape[2]
    experts = local_exp * n_ep
    side = math.isqrt(n_ep)
    slab = local_exp * cap
    chunk = side * slab
    me = lax.axis_index("ep")
    tp = lax.axis_index("tp")
    my_y, my_x = me // side, lax.rem(me, side)

    barrier = pltpu.get_barrier_semaphore()
    pl.semaphore_signal(barrier, inc=1, device_id={"tp": 1 - tp}, device_id_type=MESH)

    def greet(i, carry):
        peer = lax.rem(me + i, n_ep)
        pl.semaphore_signal(barrier, inc=1, device_id={"ep": peer}, device_id_type=MESH)
        return carry

    lax.fori_loop(1, n_ep, greet, 0)

    pairs = ((s_gate, sg), (s_up, su), (s_down, sd), (w_gate, wg), (w_up, wu), (w_down, wd))
    local = [
        pltpu.make_async_copy(src, dst.at[tp], local_sem.at[i])
        for i, (src, dst) in enumerate(pairs)
    ]
    remote = [
        pltpu.make_async_remote_copy(
            src_ref=src,
            dst_ref=dst.at[tp],
            send_sem=w_send.at[i],
            recv_sem=w_recv.at[i],
            device_id={"tp": 1 - tp},
            device_id_type=MESH,
        )
        for i, (src, dst) in enumerate(pairs)
    ]
    for copy in local:
        copy.start()

    step = min(32, n_rows)

    def norm(i, carry):
        rows = pl.ds(pl.multiple_of(i * step, step), step)
        xf = tokens[rows, :].astype(F32)
        scale = lax.rsqrt(jnp.mean(xf * xf, axis=-1, keepdims=True) + 1e-06)
        normed[rows, :] = (xf * scale * gain[...]).astype(BF16)
        return carry

    lax.fori_loop(0, n_rows // step, norm, 0)

    expert_of = lax.broadcasted_iota(jnp.int32, (n_rows, experts), 1)
    picks = [ids[:, k : k + 1] == expert_of for k in range(topk)]
    used = sum(p.astype(F32) for p in picks)
    earlier = (
        lax.broadcasted_iota(jnp.int32, (n_rows, n_rows), 1)
        < lax.broadcasted_iota(jnp.int32, (n_rows, n_rows), 0)
    ).astype(F32)
    place = jnp.dot(earlier.astype(BF16), used.astype(BF16), preferred_element_type=F32)
    place = place + (expert_of * cap).astype(F32)
    row_col = [
        jnp.sum(jnp.where(p, place, 0.0), axis=1, keepdims=True).astype(jnp.int32) for p in picks
    ]
    expert_of_t = lax.broadcasted_iota(jnp.int32, (experts, n_rows), 0)
    picks_t = [ids_t[k : k + 1, :] == expert_of_t for k in range(topk)]
    used_t = sum(p.astype(F32) for p in picks_t)
    earlier_t = (
        lax.broadcasted_iota(jnp.int32, (n_rows, n_rows), 0)
        < lax.broadcasted_iota(jnp.int32, (n_rows, n_rows), 1)
    ).astype(F32)
    place_t = jnp.dot(used_t.astype(BF16), earlier_t.astype(BF16), preferred_element_type=F32)
    place_t = place_t + (expert_of_t * cap).astype(F32)
    row_lane = [
        jnp.sum(jnp.where(p, place_t, 0.0), axis=0, keepdims=True).astype(jnp.int32)
        for p in picks_t
    ]

    pl.semaphore_wait(barrier, n_ep)
    for copy in remote:
        copy.start()

    def line_of(k, sign):
        return lax.rem(my_y + sign * k + side, side)

    def order(i):
        return lax.rem(jnp.where(lax.rem(i, 2) == 1, (i + 1) // 2, side - i // 2), side)

    def go(y, x, k):
        peer = y * side + x
        return pltpu.make_async_remote_copy(
            src_ref=sent.at[peer],
            dst_ref=arrived.at[me],
            send_sem=go_send.at[k],
            recv_sem=go_recv.at[k],
            device_id={"ep": peer},
            device_id_type=MESH,
        )

    def back(y, x, k):
        peer = y * side + x
        return pltpu.make_async_remote_copy(
            src_ref=results.at[peer],
            dst_ref=returned.at[me],
            send_sem=back_send.at[k],
            recv_sem=back_recv.at[k],
            device_id={"ep": peer},
            device_id_type=MESH,
        )

    def to_line(copy_of, y, k):
        def one(j, carry):
            copy_of(y, lax.rem(my_x + j, side), k).start()
            return carry

        @pl.when(k == 0)
        def _():
            lax.fori_loop(1, side, one, 0)

        @pl.when(k != 0)
        def _():
            lax.fori_loop(0, side, one, 0)

    def wait_line(buffer, sem, count):
        part = buffer.at[pl.ds(0, count)]
        pltpu.make_async_copy(part, part, sem).wait()

    def dispatch(i, carry):
        k = order(i)
        y = line_of(k, 1)
        row = lax.broadcasted_iota(jnp.int32, (chunk, n_rows), 0) + y * chunk
        pick = functools.reduce(jnp.logical_or, [row == lane for lane in row_lane])
        pick = pick.astype(F32).astype(BF16)
        for at in range(0, width, 512):
            part = jnp.dot(pick, normed[:, at : at + 512], preferred_element_type=F32)
            sent[pl.ds(pl.multiple_of(y * side, side), side), :, at : at + 512] = part.astype(
                BF16
            ).reshape(side, slab, 512)
        to_line(go, y, k)
        return carry

    lax.fori_loop(0, side, dispatch, 0)
    own = pltpu.make_async_copy(sent.at[me], arrived.at[me], go_recv.at[0])
    own.start()

    for copy in local:
        copy.wait()
    for copy in remote:
        copy.wait_recv()

    tile = min(256, n_rows)

    def shared(i, carry):
        rows = pl.ds(pl.multiple_of(i * tile, tile), tile)
        x = normed[rows, :]
        parts = []
        for h in range(2):
            first = jnp.dot(x, sg[h], preferred_element_type=F32)
            second = jnp.dot(x, su[h], preferred_element_type=F32)
            parts.append(silu_mul(first, second).astype(BF16))
        hid = jnp.concatenate(parts, axis=1)

        def down(n, carry):
            cols = pl.ds(pl.multiple_of(n * 256, 256), 256)
            w = sd[:, :, cols].reshape(2 * sd.shape[1], 256)
            total[rows, cols] = jnp.dot(hid, w, preferred_element_type=F32)
            return carry

        return lax.fori_loop(0, width // 256, down, carry)

    lax.fori_loop(0, n_rows // tile, shared, 0)

    expert_row = lax.rem(
        lax.broadcasted_iota(jnp.int32, (chunk, half), 0) // cap, local_exp
    )

    def experts_of(i, carry):
        k = order(i)
        y = line_of(k, -1)
        wait_line(arrived, go_recv.at[k], side)
        lines = pl.ds(pl.multiple_of(y * side, side), side)
        x = arrived[lines].reshape(chunk, width)

        def up(m, carry):
            h, j = m // local_exp, lax.rem(m, local_exp)
            first = jnp.dot(x, wg[h, j], preferred_element_type=F32)
            second = jnp.dot(x, wu[h, j], preferred_element_type=F32)
            both = jnp.where(expert_row == j, silu_mul(first, second), 0.0)
            hidden[:, pl.ds(pl.multiple_of(m * half, half), half)] = both.astype(BF16)
            return carry

        lax.fori_loop(0, 2 * local_exp, up, 0)

        def down(n, carry):
            cols = pl.ds(pl.multiple_of(n * 256, 256), 256)
            w = wd[:, :, :, cols].reshape(2 * local_exp * half, 256)
            part = jnp.dot(hidden[...], w, preferred_element_type=F32)
            results[lines, :, cols] = part.astype(BF16).reshape(side, slab, 256)
            return carry

        lax.fori_loop(0, width // 256, down, 0)
        to_line(back, y, k)
        return carry

    lax.fori_loop(0, side, experts_of, 0)
    pltpu.make_async_copy(results.at[me], returned.at[me], back_recv.at[0]).start()

    def combine(i, carry):
        k = order(i)
        y = line_of(k, 1)
        wait_line(returned, back_recv.at[k], side)
        row = lax.broadcasted_iota(jnp.int32, (n_rows, chunk), 1) + y * chunk
        weight = sum(
            jnp.where(row == row_col[j], gates[:, j : j + 1], 0.0) for j in range(topk)
        )
        high = weight.astype(BF16)
        low = (weight - high.astype(F32)).astype(BF16)
        lines = pl.ds(pl.multiple_of(y * side, side), side)

        def add(n, carry):
            cols = pl.ds(pl.multiple_of(n * 256, 256), 256)
            part = returned[lines, :, cols].reshape(chunk, 256)
            total[:, cols] += jnp.dot(high, part, preferred_element_type=F32) + jnp.dot(
                low, part, preferred_element_type=F32
            )
            return carry

        return lax.fori_loop(0, width // 256, add, carry)

    lax.fori_loop(0, side, combine, 0)

    def finish(i, carry):
        rows = pl.ds(pl.multiple_of(i * step, step), step)
        out[rows, :] = total[rows, :].astype(BF16)
        return carry

    lax.fori_loop(0, n_rows // step, finish, 0)

    for copy in remote:
        copy.wait_send()
    for k in range(side):
        count = side - 1 if k == 0 else side
        wait_line(sent, go_send.at[k], count)
        wait_line(results, back_send.at[k], count)


def body(n_ep, tokens, norm_gain, expert_ids, gate_values, w_gate, w_up, w_down, s_gate, s_up, s_down):
    n_rows, width = tokens.shape
    topk = expert_ids.shape[1]
    local_exp, _, half = w_gate.shape
    experts = local_exp * n_ep
    cap = 2 * n_rows * topk // experts
    side = math.isqrt(n_ep)
    slab = local_exp * cap
    chunk = side * slab
    vmem = pl.BlockSpec(memory_space=pltpu.VMEM)
    hbm = pl.BlockSpec(memory_space=pl.ANY)
    slabs = pltpu.VMEM((n_ep, slab, width), BF16)
    dma = pltpu.SemaphoreType.DMA
    return pl.pallas_call(
        functools.partial(kernel, n_ep, topk, cap),
        out_shape=jax.ShapeDtypeStruct((n_rows, width), BF16),
        in_specs=[vmem] * 5 + [hbm] * 6,
        out_specs=vmem,
        scratch_shapes=[
            pltpu.VMEM((n_rows, width), BF16),
            slabs,
            slabs,
            slabs,
            slabs,
            pltpu.VMEM((chunk, 2 * local_exp * half), BF16),
            pltpu.VMEM((n_rows, width), F32),
            pltpu.VMEM((2,) + w_gate.shape, BF16),
            pltpu.VMEM((2,) + w_up.shape, BF16),
            pltpu.VMEM((2,) + w_down.shape, BF16),
            pltpu.VMEM((2,) + s_gate.shape, BF16),
            pltpu.VMEM((2,) + s_up.shape, BF16),
            pltpu.VMEM((2,) + s_down.shape, BF16),
            dma((6,)),
            dma((6,)),
            dma((6,)),
            dma((side,)),
            dma((side,)),
            dma((side,)),
            dma((side,)),
        ],
        compiler_params=pltpu.CompilerParams(
            collective_id=0, has_side_effects=True, vmem_limit_bytes=58 * 1024 * 1024
        ),
    )(
        tokens,
        norm_gain.reshape(1, width),
        expert_ids,
        expert_ids.T,
        gate_values,
        w_gate,
        w_up,
        w_down,
        s_gate,
        s_up,
        s_down,
    )


def solution(mesh):
    return jax.shard_map(
        functools.partial(body, mesh.shape["ep"]),
        mesh=mesh,
        in_specs=(
            P(("grp", "ep", "tp"), None),
            P(),
            P(("grp", "ep", "tp"), None),
            P(("grp", "ep", "tp"), None),
            P("ep", None, "tp"),
            P("ep", None, "tp"),
            P("ep", "tp", None),
            P(None, "tp"),
            P(None, "tp"),
            P("tp", None),
        ),
        out_specs=P(("grp", "ep", "tp"), None),
        check_vma=False,
    )
```

```python
import functools
import math

import jax
import jax.numpy as jnp
from jax import lax
from jax.experimental import pallas as pl
from jax.experimental.pallas import tpu as pltpu
from jax.sharding import PartitionSpec as P

MESH = pl.DeviceIdType.MESH
BF16, F32 = jnp.bfloat16, jnp.float32


def silu_mul(first, second):
    return first * (1.0 / (1.0 + jnp.exp(-first))) * second


def kernel(
    n_ep,
    topk,
    cap,
    tokens,
    gain,
    ids_t,
    gates_t,
    w_gate,
    w_up,
    w_down,
    s_gate,
    s_up,
    s_down,
    out,
    normed,
    packed,
    passing,
    arrived,
    results,
    passing_back,
    returned,
    total,
    wg,
    wu,
    wd,
    sg,
    su,
    sd,
    local_sem,
    w_send,
    w_recv,
    send_sem,
    recv_sem,
):
    n_rows, width = tokens.shape
    local_exp = w_gate.shape[0]
    half = w_gate.shape[2]
    experts = local_exp * n_ep
    side = math.isqrt(n_ep)
    line = side * cap
    me = lax.axis_index("ep")
    tp = lax.axis_index("tp")
    at = (lax.rem(me, side), me // side)

    def peer(axis, pos):
        return at[1] * side + pos if axis == 0 else pos * side + at[0]

    barrier = pltpu.get_barrier_semaphore()
    pl.semaphore_signal(barrier, inc=1, device_id={"tp": 1 - tp}, device_id_type=MESH)
    for axis in range(2):

        def greet(i, carry):
            to = peer(axis, lax.rem(at[axis] + i, side))
            pl.semaphore_signal(barrier, inc=1, device_id={"ep": to}, device_id_type=MESH)
            return carry

        lax.fori_loop(1, side, greet, 0)

    pairs = ((s_gate, sg), (s_up, su), (s_down, sd), (w_gate, wg), (w_up, wu), (w_down, wd))
    local = [
        pltpu.make_async_copy(src, dst.at[tp], local_sem.at[i])
        for i, (src, dst) in enumerate(pairs)
    ]
    remote = [
        pltpu.make_async_remote_copy(
            src_ref=src,
            dst_ref=dst.at[tp],
            send_sem=w_send.at[i],
            recv_sem=w_recv.at[i],
            device_id={"tp": 1 - tp},
            device_id_type=MESH,
        )
        for i, (src, dst) in enumerate(pairs)
    ]
    for copy in local:
        copy.start()

    step = min(32, n_rows)

    def norm(i, carry):
        rows = pl.ds(pl.multiple_of(i * step, step), step)
        xf = tokens[rows, :].astype(F32)
        scale = lax.rsqrt(jnp.mean(xf * xf, axis=-1, keepdims=True) + 1e-06)
        normed[rows, :] = (xf * scale * gain[...]).astype(BF16)
        return carry

    lax.fori_loop(0, n_rows // step, norm, 0)

    expert_of = lax.broadcasted_iota(jnp.int32, (experts, n_rows), 0)
    device_of, j_of = expert_of // local_exp, lax.rem(expert_of, local_exp)
    x_of, y_of = lax.rem(device_of, side), device_of // side
    flip = lax.rem(j_of, 2) == 1
    first_row = j_of * n_ep + jnp.where(flip, y_of * side + x_of, x_of * side + y_of)
    picks = [ids_t[k : k + 1, :] == expert_of for k in range(topk)]
    used = sum(p.astype(F32) for p in picks).astype(BF16)
    earlier = (
        lax.broadcasted_iota(jnp.int32, (n_rows, n_rows), 0)
        < lax.broadcasted_iota(jnp.int32, (n_rows, n_rows), 1)
    ).astype(F32).astype(BF16)
    place = jnp.dot(used, earlier, preferred_element_type=F32) + (first_row * cap).astype(F32)
    row_f = [jnp.sum(jnp.where(p, place, 0.0), axis=0, keepdims=True) for p in picks]
    row_lane = [r.astype(jnp.int32) for r in row_f]
    packed_cols = jnp.concatenate(
        row_f
        + [gates_t[k : k + 1, :] for k in range(topk)]
        + [jnp.zeros((8 - 2 * topk, n_rows), F32)],
        axis=0,
    ).T
    row_col = [packed_cols[:, k : k + 1].astype(jnp.int32) for k in range(topk)]
    gate_col = [packed_cols[:, topk + k : topk + k + 1] for k in range(topk)]

    pl.semaphore_wait(barrier, 2 * side - 1)
    for copy in remote:
        copy.start()

    def order(i):
        i = lax.rem(i + 1, side)
        return lax.rem(jnp.where(lax.rem(i, 2) == 1, (i + 1) // 2, side - i // 2), side)

    def axis_of(phase, j):
        return (j + phase + phase // 2) % 2

    def send(phase, j, pos, src, dst):
        axis = axis_of(phase, j)
        mine = at[axis]
        sem = recv_sem.at[phase, j, mine]

        @pl.when(pos == mine)
        def _():
            pltpu.make_async_copy(src, dst, sem).start()

        @pl.when(pos != mine)
        def _():
            pltpu.make_async_remote_copy(
                src_ref=src,
                dst_ref=dst,
                send_sem=send_sem.at[phase, j],
                recv_sem=sem,
                device_id={"ep": peer(axis, pos)},
                device_id_type=MESH,
            ).start()

    def arrival(phase, j, pos):
        part = packed.at[j, 0]
        pltpu.make_async_copy(part, part, recv_sem.at[phase, j, pos]).wait()

    def dispatch(i, carry):
        for j in range(local_exp):
            axis = axis_of(0, j)
            pos = lax.rem(at[axis] + order(i), side)
            row = lax.broadcasted_iota(jnp.int32, (line, n_rows), 0) + (j * side + pos) * line
            pick = functools.reduce(jnp.logical_or, [row == lane for lane in row_lane])
            pick = pick.astype(F32).astype(BF16)
            for col in range(0, width, 512):
                part = jnp.dot(pick, normed[:, col : col + 512], preferred_element_type=F32)
                packed[j, pos, :, :, col : col + 512] = part.reshape(side, cap, 512).astype(BF16)
            send(0, j, pos, packed.at[j, pos], passing.at[j, :, at[axis]])
        return carry

    lax.fori_loop(0, side, dispatch, 0)

    for copy in local:
        copy.wait()
    for copy in remote:
        copy.wait_recv()

    x = normed[...]
    parts = []
    for h in range(2):
        first = jnp.dot(x, sg[h], preferred_element_type=F32)
        second = jnp.dot(x, su[h], preferred_element_type=F32)
        parts.append(silu_mul(first, second).astype(BF16))
    hid = jnp.concatenate(parts, axis=1)

    def shared_down(n, carry):
        cols = pl.ds(pl.multiple_of(n * 256, 256), 256)
        w = sd[:, :, cols].reshape(2 * sd.shape[1], 256)
        total[:, cols] = jnp.dot(hid, w, preferred_element_type=F32)
        return carry

    lax.fori_loop(0, width // 256, shared_down, 0)

    def turn(phase, source, target):
        for j in range(local_exp):

            def landed(pos, carry):
                arrival(phase - 1, j, pos)
                return carry

            lax.fori_loop(0, side, landed, 0)
            axis = axis_of(phase, j)

            def forward(i, carry):
                pos = lax.rem(at[axis] + order(i), side)
                send(phase, j, pos, source.at[j, pos], target(j, at[axis]))
                return carry

            lax.fori_loop(0, side, forward, 0)

    turn(1, passing, lambda j, mine: arrived.at[j, mine])

    def experts_of(i, carry):
        for j in range(local_exp):
            axis = axis_of(1, j)
            pos = lax.rem(at[axis] - order(i) + side, side)
            arrival(1, j, pos)
            x = arrived[j, pos].reshape(line, width)
            parts = []
            for h in range(2):
                first = jnp.dot(x, wg[h, j], preferred_element_type=F32)
                second = jnp.dot(x, wu[h, j], preferred_element_type=F32)
                parts.append(silu_mul(first, second).astype(BF16))
            hid = jnp.concatenate(parts, axis=1)
            for col in range(0, width, 512):
                w = wd[:, j, :, col : col + 512].reshape(2 * half, 512)
                part = jnp.dot(hid, w, preferred_element_type=F32)
                results[j, pos, :, :, col : col + 512] = part.reshape(side, cap, 512).astype(BF16)
            send(2, j, pos, results.at[j, pos], passing_back.at[j, :, at[axis]])
        return carry

    lax.fori_loop(0, side, experts_of, 0)

    turn(3, passing_back, lambda j, mine: returned.at[j, mine])

    def combine(i, carry):
        weights, rows = [], []
        for j in range(local_exp):
            axis = axis_of(3, j)
            pos = lax.rem(at[axis] - order(i) + side, side)
            arrival(3, j, pos)
            row = lax.broadcasted_iota(jnp.int32, (n_rows, line), 1) + (j * side + pos) * line
            weight = sum(
                jnp.where(row == row_col[k], gate_col[k], 0.0) for k in range(topk)
            )
            high = weight.astype(BF16)
            weights += [high, (weight - high.astype(F32)).astype(BF16)]
            rows += [(j, pos)] * 2
        weights = jnp.concatenate(weights, axis=1)
        for col in range(0, width, 256):
            part = jnp.concatenate(
                [
                    returned[j, pos, :, :, col : col + 256].reshape(line, 256)
                    for j, pos in rows
                ],
                axis=0,
            )
            total[:, col : col + 256] += jnp.dot(weights, part, preferred_element_type=F32)
        return carry

    lax.fori_loop(0, side, combine, 0)

    def finish(i, carry):
        rows = pl.ds(pl.multiple_of(i * step, step), step)
        out[rows, :] = total[rows, :].astype(BF16)
        return carry

    lax.fori_loop(0, n_rows // step, finish, 0)

    for copy in remote:
        copy.wait_send()
    for phase in range(4):
        for j in range(local_exp):
            part = packed.at[j, pl.ds(0, side - 1)]
            pltpu.make_async_copy(part, part, send_sem.at[phase, j]).wait()


def body(n_ep, tokens, norm_gain, expert_ids, gate_values, w_gate, w_up, w_down, s_gate, s_up, s_down):
    n_rows, width = tokens.shape
    topk = expert_ids.shape[1]
    local_exp, _, half = w_gate.shape
    experts = local_exp * n_ep
    cap = 2 * n_rows * topk // experts
    side = math.isqrt(n_ep)
    vmem = pl.BlockSpec(memory_space=pltpu.VMEM)
    hbm = pl.BlockSpec(memory_space=pl.ANY)
    rows = pltpu.VMEM((local_exp, side, side, cap, width), BF16)
    dma = pltpu.SemaphoreType.DMA
    return pl.pallas_call(
        functools.partial(kernel, n_ep, topk, cap),
        out_shape=jax.ShapeDtypeStruct((n_rows, width), BF16),
        in_specs=[vmem] * 4 + [hbm] * 6,
        out_specs=vmem,
        scratch_shapes=[pltpu.VMEM((n_rows, width), BF16)]
        + [rows] * 6
        + [pltpu.VMEM((n_rows, width), F32)]
        + [
            pltpu.VMEM((2,) + w.shape, BF16)
            for w in (w_gate, w_up, w_down, s_gate, s_up, s_down)
        ]
        + [dma((6,))] * 3
        + [dma((4, local_exp)), dma((4, local_exp, side))],
        compiler_params=pltpu.CompilerParams(
            collective_id=0, has_side_effects=True, vmem_limit_bytes=60 * 1024 * 1024
        ),
    )(
        tokens,
        norm_gain.reshape(1, width),
        expert_ids.T,
        gate_values.T,
        w_gate,
        w_up,
        w_down,
        s_gate,
        s_up,
        s_down,
    )


def solution(mesh):
    return jax.shard_map(
        functools.partial(body, mesh.shape["ep"]),
        mesh=mesh,
        in_specs=(
            P(("grp", "ep", "tp"), None),
            P(),
            P(("grp", "ep", "tp"), None),
            P(("grp", "ep", "tp"), None),
            P("ep", None, "tp"),
            P("ep", None, "tp"),
            P("ep", "tp", None),
            P(None, "tp"),
            P(None, "tp"),
            P("tp", None),
        ),
        out_specs=P(("grp", "ep", "tp"), None),
        check_vma=False,
    )
```

```python
import functools
import math

import jax
import jax.numpy as jnp
from jax import lax
from jax.experimental import pallas as pl
from jax.experimental.pallas import tpu as pltpu
from jax.sharding import PartitionSpec as P

MESH = pl.DeviceIdType.MESH
BF16, F32 = jnp.bfloat16, jnp.float32


def silu_mul(first, second):
    return first * (1.0 / (1.0 + jnp.exp(-first))) * second


def kernel(
    n_ep,
    topk,
    cap,
    tokens,
    gain,
    ids_t,
    gates_t,
    w_gate,
    w_up,
    w_down,
    s_gate,
    s_up,
    s_down,
    out,
    normed,
    notes_out,
    notes_in,
    dense,
    packed,
    passing,
    arrived,
    results,
    passing_back,
    packed_back,
    sums,
    dense_back,
    total,
    wg,
    wu,
    wd,
    sg,
    su,
    sd,
    local_sem,
    w_send,
    w_recv,
    note_send,
    note_recv,
    dense_send,
    dense_recv,
    relay_send,
    relay_recv,
    cross_send,
    cross_recv,
    home_send,
    home_recv,
    hub_send,
    hub_recv,
    sum_send,
    sum_recv,
):
    n_rows, width = tokens.shape
    chunks, _, cols = normed.shape
    local_exp = w_gate.shape[0]
    half = w_gate.shape[2]
    experts = local_exp * n_ep
    side = math.isqrt(n_ep)
    line = side * cap
    reach = side // 2
    me = lax.axis_index("ep")
    tp = lax.axis_index("tp")
    at = (lax.rem(me, side), me // side)

    def peer(axis, pos):
        return at[1] * side + pos if axis == 0 else pos * side + at[0]

    def ahead(axis, s, d):
        return lax.rem(at[axis] + (d if s == 0 else side - d), side)

    def first_axis(c):
        return c % 2

    barrier = pltpu.get_barrier_semaphore()
    pl.semaphore_signal(barrier, inc=1, device_id={"tp": 1 - tp}, device_id_type=MESH)
    for axis in range(2):

        def greet(i, carry):
            to = peer(axis, lax.rem(at[axis] + i, side))
            pl.semaphore_signal(barrier, inc=1, device_id={"ep": to}, device_id_type=MESH)
            return carry

        lax.fori_loop(1, side, greet, 0)

    pairs = ((s_gate, sg), (s_up, su), (s_down, sd), (w_gate, wg), (w_up, wu), (w_down, wd))
    local = [
        pltpu.make_async_copy(src, dst.at[tp], local_sem.at[i])
        for i, (src, dst) in enumerate(pairs)
    ]
    remote = [
        pltpu.make_async_remote_copy(
            src_ref=src,
            dst_ref=dst.at[tp],
            send_sem=w_send.at[i],
            recv_sem=w_recv.at[i],
            device_id={"tp": 1 - tp},
            device_id_type=MESH,
        )
        for i, (src, dst) in enumerate(pairs)
    ]
    for copy in local:
        copy.start()

    step = min(32, n_rows)

    def norm(i, carry):
        rows = pl.ds(pl.multiple_of(i * step, step), step)
        xf = tokens[rows, :].astype(F32)
        scale = lax.rsqrt(jnp.mean(xf * xf, axis=-1, keepdims=True) + 1e-06)
        done = (xf * scale * gain[...]).astype(BF16)
        for c in range(chunks):
            normed[c, rows, :] = done[:, c * cols : (c + 1) * cols]
        return carry

    lax.fori_loop(0, n_rows // step, norm, 0)

    pl.semaphore_wait(barrier, 2 * side - 1)

    def to_peer(axis, pos, src, dst, send_sem, recv_sem):
        pltpu.make_async_remote_copy(
            src_ref=src,
            dst_ref=dst,
            send_sem=send_sem,
            recv_sem=recv_sem,
            device_id={"ep": peer(axis, pos)},
            device_id_type=MESH,
        ).start()

    def wait_for(part, sem):
        pltpu.make_async_copy(part, part, sem).wait()

    def send_dense(c):
        for s in range(2):
            axis = first_axis(c)
            to_peer(
                axis,
                ahead(axis, s, 1),
                normed.at[c],
                dense.at[c, s],
                dense_send.at[c],
                dense_recv.at[c, s],
            )

    send_dense(0)
    send_dense(1)

    expert_of = lax.broadcasted_iota(jnp.int32, (experts, n_rows), 0)
    device_of, j_of = expert_of // local_exp, lax.rem(expert_of, local_exp)
    x_of, y_of = lax.rem(device_of, side), device_of // side
    picks = [ids_t[k : k + 1, :] == expert_of for k in range(topk)]
    used = sum(p.astype(F32) for p in picks).astype(BF16)
    earlier = (
        lax.broadcasted_iota(jnp.int32, (n_rows, n_rows), 0)
        < lax.broadcasted_iota(jnp.int32, (n_rows, n_rows), 1)
    ).astype(F32).astype(BF16)
    slot = jnp.dot(used, earlier, preferred_element_type=F32)
    blank = jnp.zeros((8 - 2 * topk, n_rows), F32)
    for axis in range(2):
        pair = x_of * side + y_of if axis == 0 else y_of * side + x_of
        place = slot + ((j_of * n_ep + pair) * cap).astype(F32)
        notes_out[axis] = jnp.concatenate(
            [jnp.sum(jnp.where(p, place, 0.0), axis=0, keepdims=True) for p in picks]
            + [gates_t[k : k + 1, :] for k in range(topk)]
            + [blank],
            axis=0,
        )
    for axis in range(2):
        for s in range(2):
            to_peer(
                axis,
                ahead(axis, s, 1),
                notes_out.at[axis],
                notes_in.at[axis, s],
                note_send.at[0],
                note_recv.at[axis, s],
            )
    for c in range(2, chunks):
        send_dense(c)
    for copy in remote:
        copy.start()

    def pick_rows(notes, row):
        lanes = [notes[k : k + 1, :].astype(jnp.int32) for k in range(topk)]
        pick = functools.reduce(jnp.logical_or, [row == lane for lane in lanes])
        return pick.astype(F32).astype(BF16)

    def weigh_rows(notes, row):
        by_token = notes.T
        weight = sum(
            jnp.where(
                row == by_token[:, k : k + 1].astype(jnp.int32),
                by_token[:, topk + k : topk + k + 1],
                0.0,
            )
            for k in range(topk)
        )
        high = weight.astype(BF16)
        return high, (weight - high.astype(F32)).astype(BF16)

    tail = pl.ds(side // 2, side // 2), pl.ds(0, side // 2)
    for j in range(local_exp):
        for axis in range(2):
            row = lax.broadcasted_iota(jnp.int32, (line, n_rows), 0)
            pick = pick_rows(notes_out[axis], row + (j * side + at[axis]) * line)
            for c in range(axis, chunks, 2):
                part = jnp.dot(pick, normed[c], preferred_element_type=F32)
                passing[c, :, j, at[axis]] = part.reshape(side, cap, cols).astype(BF16)
    for c in range(chunks):
        for s in range(2):
            for j in range(local_exp):
                packed_back[c, s, reach - 2, j, tail[s]] = jnp.zeros(
                    (side // 2, cap, cols), BF16
                )

    parts_of = (pl.ds(0, side // 2), pl.ds(side // 2, side // 2))

    def relay(j, c):
        axis = first_axis(c)
        for s in range(2):
            if j == 0:
                wait_for(dense.at[c, s], dense_recv.at[c, s])
                if c < 2:
                    wait_for(notes_in.at[axis, s], note_recv.at[axis, s])
            source = ahead(axis, 1 - s, 1)
            i = lax.broadcasted_iota(jnp.int32, (reach * line, n_rows), 0)
            d = i // line
            pos = lax.rem(at[axis] + (d if s == 0 else side - d), side)
            row = (j * side + pos) * line + lax.rem(i, line)
            pick = pick_rows(notes_in[axis, s], row)
            part = jnp.dot(pick, dense[c, s], preferred_element_type=F32).astype(BF16)
            part = part.reshape(reach, side, cap, cols)
            packed[c, j, s] = part[1:]
            passing[c, :, j, source] = part[0]
            for d in range(1, reach):
                rows = pl.ds(0, side) if d < reach - 1 else parts_of[s]
                to_peer(
                    axis,
                    ahead(axis, s, d),
                    packed.at[c, j, s, d - 1, rows],
                    passing.at[c, rows, j, source],
                    relay_send.at[c, j],
                    relay_recv.at[c, j],
                )

    for j in range(local_exp):
        for c in range(chunks):
            relay(j, c)

    for copy in local:
        copy.wait()
    for copy in remote:
        copy.wait_recv()
    parts = []
    for h in range(2):
        first = sum(
            jnp.dot(normed[c], sg[h, c * cols : (c + 1) * cols], preferred_element_type=F32)
            for c in range(chunks)
        )
        second = sum(
            jnp.dot(normed[c], su[h, c * cols : (c + 1) * cols], preferred_element_type=F32)
            for c in range(chunks)
        )
        parts.append(silu_mul(first, second).astype(BF16))
    hid = jnp.concatenate(parts, axis=1)
    for c in range(chunks):
        w = sd[:, :, c * cols : (c + 1) * cols].reshape(2 * half, cols)
        total[c] = jnp.dot(hid, w, preferred_element_type=F32)

    def order(i):
        i = lax.rem(i + 1, side)
        return lax.rem(jnp.where(lax.rem(i, 2) == 1, (i + 1) // 2, side - i // 2), side)

    def across(j, c, source_of, target_of, send_sem, recv_sem):
        axis = 1 - first_axis(c)
        mine = at[axis]

        def one(i, carry):
            pos = lax.rem(mine + order(i), side)
            src, dst = source_of(pos), target_of(mine)

            @pl.when(pos == mine)
            def _():
                pltpu.make_async_copy(src, dst, recv_sem.at[c, j]).start()

            @pl.when(pos != mine)
            def _():
                to_peer(axis, pos, src, dst, send_sem.at[c, j], recv_sem.at[c, j])

            return carry

        lax.fori_loop(0, side, one, 0)

    def by_source(ref, j, c, pos):
        return ref.at[c, j, pos] if first_axis(c) == 0 else ref.at[c, j, :, pos]

    for j in range(local_exp):
        for c in range(chunks):
            wait_for(results.at[c, 0, pl.ds(0, side - 3)], relay_recv.at[c, j])
            across(
                j,
                c,
                lambda pos: passing.at[c, pos, j],
                lambda mine: by_source(arrived, j, c, mine),
                cross_send,
                cross_recv,
            )

    block = max(1, side // 2)
    for j in range(local_exp):
        for c in range(chunks):
            wait_for(results.at[c, 0], cross_recv.at[c, j])

        def experts_of(i, carry):
            rows = pl.ds(i * block, block)
            xs = [
                arrived[c, j, rows].reshape(block * line, cols) for c in range(chunks)
            ]
            parts = []
            for h in range(2):
                first = sum(
                    jnp.dot(xs[c], wg[h, j, c * cols : (c + 1) * cols], preferred_element_type=F32)
                    for c in range(chunks)
                )
                second = sum(
                    jnp.dot(xs[c], wu[h, j, c * cols : (c + 1) * cols], preferred_element_type=F32)
                    for c in range(chunks)
                )
                parts.append(silu_mul(first, second).astype(BF16))
            hid = jnp.concatenate(parts, axis=1)
            for c in range(chunks):
                w = wd[:, j, :, c * cols : (c + 1) * cols].reshape(2 * half, cols)
                part = jnp.dot(hid, w, preferred_element_type=F32)
                results[c, j, rows] = part.reshape(block, side, cap, cols).astype(BF16)
            return carry

        lax.fori_loop(0, side // block, experts_of, 0)
        for c in range(chunks):
            across(
                j,
                c,
                lambda pos: by_source(results, j, c, pos),
                lambda mine: passing_back.at[c, j, :, mine],
                home_send,
                home_recv,
            )

    for j in range(local_exp):
        for c in range(chunks):
            axis = first_axis(c)
            wait_for(results.at[c, 0], home_recv.at[c, j])
            for d in range(1, reach):
                for s in range(2):
                    rows = pl.ds(0, side) if d < reach - 1 else parts_of[s]
                    to_peer(
                        axis,
                        ahead(axis, 1 - s, d),
                        passing_back.at[c, j, ahead(axis, 1 - s, d + 1), rows],
                        packed_back.at[c, s, d - 1, j, rows],
                        hub_send.at[c, j],
                        hub_recv.at[c, s],
                    )

    for axis in range(2):
        i = lax.broadcasted_iota(jnp.int32, (n_rows, local_exp * line), 1)
        row = (i // line * side + at[axis]) * line + lax.rem(i, line)
        high, low = weigh_rows(notes_out[axis], row)
        for c in range(axis, chunks, 2):
            rhs = jnp.concatenate(
                [passing_back[c, j, at[axis]].reshape(line, cols) for j in range(local_exp)], axis=0
            )
            total[c] += jnp.dot(high, rhs, preferred_element_type=F32) + jnp.dot(
                low, rhs, preferred_element_type=F32
            )

    for c in range(chunks):
        axis = first_axis(c)
        for s in range(2):
            source = ahead(axis, 1 - s, 1)
            i = lax.broadcasted_iota(jnp.int32, (n_rows, reach * local_exp * line), 1)
            d = i // (local_exp * line)
            j_row = lax.rem(i // line, local_exp)
            pos = lax.rem(at[axis] + (d if s == 0 else side - d), side)
            row = (j_row * side + pos) * line + lax.rem(i, line)
            high, low = weigh_rows(notes_in[axis, s], row)
            wait_for(results.at[c, 0, pl.ds(0, side - 3)], hub_recv.at[c, s])
            rhs = jnp.concatenate(
                [passing_back[c, j, source].reshape(line, cols) for j in range(local_exp)]
                + [packed_back[c, s].reshape((reach - 1) * local_exp * line, cols)],
                axis=0,
            )
            part = jnp.dot(high, rhs, preferred_element_type=F32) + jnp.dot(
                low, rhs, preferred_element_type=F32
            )
            sums[c, s] = part.astype(BF16)
            to_peer(
                axis,
                source,
                sums.at[c, s],
                dense_back.at[c, 1 - s],
                sum_send.at[c],
                sum_recv.at[c, 1 - s],
            )

    for c in range(chunks):
        for s in range(2):
            wait_for(dense_back.at[c, s], sum_recv.at[c, s])
        mixed = total[c] + dense_back[c, 0].astype(F32) + dense_back[c, 1].astype(F32)
        out[:, c * cols : (c + 1) * cols] = mixed.astype(BF16)

    for copy in remote:
        copy.wait_send()
    wait_for(notes_in, note_send.at[0])
    for c in range(chunks):
        wait_for(dense.at[c], dense_send.at[c])
        wait_for(sums.at[c], sum_send.at[c])
        for j in range(local_exp):
            wait_for(results.at[c, 0, pl.ds(0, side - 3)], relay_send.at[c, j])
            wait_for(results.at[c, 0, pl.ds(0, side - 1)], cross_send.at[c, j])
            wait_for(results.at[c, 0, pl.ds(0, side - 1)], home_send.at[c, j])
            wait_for(results.at[c, 0, pl.ds(0, side - 3)], hub_send.at[c, j])


def body(n_ep, tokens, norm_gain, expert_ids, gate_values, w_gate, w_up, w_down, s_gate, s_up, s_down):
    n_rows, width = tokens.shape
    topk = expert_ids.shape[1]
    local_exp, _, half = w_gate.shape
    experts = local_exp * n_ep
    cap = 2 * n_rows * topk // experts
    side = math.isqrt(n_ep)
    chunks = 4
    cols = width // chunks
    reach = side // 2
    vmem = pl.BlockSpec(memory_space=pltpu.VMEM)
    hbm = pl.BlockSpec(memory_space=pl.ANY)
    dma = pltpu.SemaphoreType.DMA

    def tall(*shape):
        return pltpu.VMEM((chunks,) + shape + (cols,), BF16)

    per_expert, per_side = dma((chunks, local_exp)), dma((chunks, 2))
    return pl.pallas_call(
        functools.partial(kernel, n_ep, topk, cap),
        out_shape=jax.ShapeDtypeStruct((n_rows, width), BF16),
        in_specs=[vmem] * 4 + [hbm] * 6,
        out_specs=vmem,
        scratch_shapes=[
            tall(n_rows),
            pltpu.VMEM((2, 8, n_rows), F32),
            pltpu.VMEM((2, 2, 8, n_rows), F32),
            tall(2, n_rows),
            tall(local_exp, 2, reach - 1, side, cap),
            tall(side, local_exp, side, cap),
            tall(local_exp, side, side, cap),
            tall(local_exp, side, side, cap),
            tall(local_exp, side, side, cap),
            tall(2, reach - 1, local_exp, side, cap),
            tall(2, n_rows),
            tall(2, n_rows),
            pltpu.VMEM((chunks, n_rows, cols), F32),
        ]
        + [
            pltpu.VMEM((2,) + w.shape, BF16)
            for w in (w_gate, w_up, w_down, s_gate, s_up, s_down)
        ]
        + [dma((6,))] * 3
        + [dma((1,)), dma((2, 2)), dma((chunks,)), per_side]
        + [per_expert] * 6
        + [per_expert, per_side, dma((chunks,)), per_side],
        compiler_params=pltpu.CompilerParams(
            collective_id=0, has_side_effects=True, vmem_limit_bytes=62 * 1024 * 1024
        ),
    )(
        tokens,
        norm_gain.reshape(1, width),
        expert_ids.T,
        gate_values.T,
        w_gate,
        w_up,
        w_down,
        s_gate,
        s_up,
        s_down,
    )


def solution(mesh):
    return jax.shard_map(
        functools.partial(body, mesh.shape["ep"]),
        mesh=mesh,
        in_specs=(
            P(("grp", "ep", "tp"), None),
            P(),
            P(("grp", "ep", "tp"), None),
            P(("grp", "ep", "tp"), None),
            P("ep", None, "tp"),
            P("ep", None, "tp"),
            P("ep", "tp", None),
            P(None, "tp"),
            P(None, "tp"),
            P("tp", None),
        ),
        out_specs=P(("grp", "ep", "tp"), None),
        check_vma=False,
    )
```

```python
import functools
import math

import jax
import jax.numpy as jnp
from jax import lax
from jax.experimental import pallas as pl
from jax.experimental.pallas import tpu as pltpu
from jax.sharding import PartitionSpec as P

MESH = pl.DeviceIdType.MESH
BF16, F32 = jnp.bfloat16, jnp.float32
VMEM_MIB = 62


def silu_mul(first, second):
    return first * (1.0 / (1.0 + jnp.exp(-first))) * second


def kernel(
    n_ep,
    topk,
    cap,
    tokens,
    gain,
    ids_t,
    gates_t,
    w_gate,
    w_up,
    w_down,
    s_gate,
    s_up,
    s_down,
    out,
    normed,
    notes_out,
    notes_in,
    dense,
    dense_far,
    packed,
    passing,
    arrived,
    passing_back,
    packed_back,
    chain,
    dense_back,
    total,
    wg,
    wu,
    wd,
    sg,
    su,
    sd,
    local_sem,
    w_send,
    w_recv,
    note_send,
    note_recv,
    dense_send,
    dense_recv,
    far_send,
    far_recv,
    relay_send,
    relay_recv,
    cross_send,
    cross_recv,
    home_send,
    home_recv,
    hub_send,
    hub_recv,
    chain_send,
    chain_recv,
    sum_send,
    sum_recv,
):
    n_rows, width = tokens.shape
    chunks, _, cols = normed.shape
    local_exp = w_gate.shape[0]
    half = w_gate.shape[2]
    experts = local_exp * n_ep
    side = math.isqrt(n_ep)
    line = side * cap
    reach = side // 2 - 1
    relayed = max(0, 2 * reach - 3)
    me = lax.axis_index("ep")
    tp = lax.axis_index("tp")
    at = (lax.rem(me, side), me // side)

    def peer(axis, pos):
        return at[1] * side + pos if axis == 0 else pos * side + at[0]

    def ahead(axis, s, d):
        return lax.rem(at[axis] + (d if s == 0 else side - d), side)

    def first_axis(c):
        return c % 2

    def span(distance, s):
        if distance < side // 2:
            return pl.ds(0, side)
        return pl.ds(s * (side // 2), side // 2)

    barrier = pltpu.get_barrier_semaphore()
    pl.semaphore_signal(barrier, inc=1, device_id={"tp": 1 - tp}, device_id_type=MESH)
    for axis in range(2):

        def greet(i, carry):
            to = peer(axis, lax.rem(at[axis] + i, side))
            pl.semaphore_signal(barrier, inc=1, device_id={"ep": to}, device_id_type=MESH)
            return carry

        lax.fori_loop(1, side, greet, 0)

    pairs = ((s_gate, sg), (s_up, su), (s_down, sd), (w_gate, wg), (w_up, wu), (w_down, wd))
    local = [
        pltpu.make_async_copy(src, dst.at[tp], local_sem.at[i])
        for i, (src, dst) in enumerate(pairs)
    ]
    remote = [
        pltpu.make_async_remote_copy(
            src_ref=src,
            dst_ref=dst.at[tp],
            send_sem=w_send.at[i],
            recv_sem=w_recv.at[i],
            device_id={"tp": 1 - tp},
            device_id_type=MESH,
        )
        for i, (src, dst) in enumerate(pairs)
    ]
    for copy in local:
        copy.start()

    pl.semaphore_wait(barrier, 2 * side - 1)

    def to_peer(axis, pos, src, dst, send_sem, recv_sem):
        pltpu.make_async_remote_copy(
            src_ref=src,
            dst_ref=dst,
            send_sem=send_sem,
            recv_sem=recv_sem,
            device_id={"ep": peer(axis, pos)},
            device_id_type=MESH,
        ).start()

    def wait_for(part, sem):
        pltpu.make_async_copy(part, part, sem).wait()

    def send_dense(c):
        for s in range(2):
            axis = first_axis(c)
            to_peer(
                axis,
                ahead(axis, s, 1),
                tokens.at[:, c * cols : (c + 1) * cols],
                dense.at[c, s],
                dense_send.at[c],
                dense_recv.at[c, s],
            )

    send_dense(0)
    send_dense(1)

    expert_of = lax.broadcasted_iota(jnp.int32, (experts, n_rows), 0)
    device_of, j_of = expert_of // local_exp, lax.rem(expert_of, local_exp)
    x_of, y_of = lax.rem(device_of, side), device_of // side
    picks = [ids_t[k : k + 1, :] == expert_of for k in range(topk)]
    used = sum(p.astype(F32) for p in picks).astype(BF16)
    earlier = (
        lax.broadcasted_iota(jnp.int32, (n_rows, n_rows), 0)
        < lax.broadcasted_iota(jnp.int32, (n_rows, n_rows), 1)
    ).astype(F32).astype(BF16)
    slot = jnp.dot(used, earlier, preferred_element_type=F32)
    blank = jnp.zeros((8 - 2 * topk, n_rows), F32)
    for axis in range(2):
        pair = x_of * side + y_of if axis == 0 else y_of * side + x_of
        place = slot + ((j_of * n_ep + pair) * cap).astype(F32)
        notes_out[axis] = jnp.concatenate(
            [jnp.sum(jnp.where(p, place, 0.0), axis=0, keepdims=True) for p in picks]
            + [gates_t[k : k + 1, :] for k in range(topk)]
            + [blank],
            axis=0,
        )
    for axis in range(2):
        for s in range(2):
            for far in range(2):
                to_peer(
                    axis,
                    ahead(axis, s, far + 1),
                    notes_out.at[axis],
                    notes_in.at[axis, s, far],
                    note_send.at[0],
                    note_recv.at[axis, s, far],
                )
    for c in range(2, chunks):
        send_dense(c)
    for copy in remote:
        copy.start()

    def pick_rows(notes, row):
        lanes = [notes[k : k + 1, :].astype(jnp.int32) for k in range(topk)]
        pick = functools.reduce(jnp.logical_or, [row == lane for lane in lanes])
        return pick.astype(F32).astype(BF16)

    def weigh_rows(notes, row):
        by_token = notes.T
        weight = sum(
            jnp.where(
                row == by_token[:, k : k + 1].astype(jnp.int32),
                by_token[:, topk + k : topk + k + 1],
                0.0,
            )
            for k in range(topk)
        )
        high = weight.astype(BF16)
        return high, (weight - high.astype(F32)).astype(BF16)

    def pick_own(notes, axis):
        i = lax.broadcasted_iota(jnp.int32, (local_exp * line, n_rows), 0)
        row = (i // line * side + at[axis]) * line + lax.rem(i, line)
        return pick_rows(notes, row)

    def keep_own(pick, source, pos, c):
        part = jnp.dot(pick, source, preferred_element_type=F32).astype(BF16)
        part = part.reshape(local_exp, side, cap, cols)
        for j in range(local_exp):
            passing[c, :, j, pos] = part[j]

    for axis in range(2):
        pick = pick_own(notes_out[axis], axis)
        for c in range(axis, chunks, 2):
            part = tokens[:, c * cols : (c + 1) * cols]
            keep_own(pick, part, at[axis], c)
    if reach > 1:
        for c in range(chunks):
            for s in range(2):
                for j in range(local_exp):
                    packed_back[c, s, reach - 2, j, span(side // 2, 1 - s)] = jnp.zeros(
                        (side // 2, cap, cols), BF16
                    )

    for c in range(chunks):
        axis = first_axis(c)
        for s in range(2):
            wait_for(dense.at[c, s], dense_recv.at[c, s])
            to_peer(
                axis,
                ahead(axis, s, 1),
                dense.at[c, s],
                dense_far.at[c, s],
                far_send.at[c],
                far_recv.at[c, s],
            )
        for s in range(2):
            if c < 2:
                wait_for(notes_in.at[axis, s, 0], note_recv.at[axis, s, 0])
            pick = pick_own(notes_in[axis, s, 0], axis)
            keep_own(pick, dense[c, s], ahead(axis, 1 - s, 1), c)

    def relay(j, c):
        axis = first_axis(c)
        for s in range(2):
            if j == 0:
                wait_for(dense_far.at[c, s], far_recv.at[c, s])
                if c < 2:
                    wait_for(notes_in.at[axis, s, 1], note_recv.at[axis, s, 1])
            source = ahead(axis, 1 - s, 2)
            i = lax.broadcasted_iota(jnp.int32, (reach * line, n_rows), 0)
            d = i // line
            pos = lax.rem(at[axis] + (d if s == 0 else side - d), side)
            row = (j * side + pos) * line + lax.rem(i, line)
            pick = pick_rows(notes_in[axis, s, 1], row)
            part = jnp.dot(pick, dense_far[c, s], preferred_element_type=F32).astype(BF16)
            part = part.reshape(reach, side, cap, cols)
            if reach > 1:
                packed[c, j, s] = part[1:]
            rows = span(2, s)
            passing[c, rows, j, source] = part[0, rows.start : rows.start + rows.size]
            for d in range(1, reach):
                rows = span(d + 2, s)
                to_peer(
                    axis,
                    ahead(axis, s, d),
                    packed.at[c, j, s, d - 1, rows],
                    passing.at[c, rows, j, source],
                    relay_send.at[c, j],
                    relay_recv.at[c, j],
                )

    for j in range(local_exp):
        for c in range(chunks):
            relay(j, c)

    step = min(32, n_rows)

    def scaled(parts):
        square = sum(jnp.sum(p * p, axis=-1, keepdims=True) for p in parts)
        scale = lax.rsqrt(square * (1.0 / width) + 1e-06)
        return [
            (p * scale * gain[:, c * cols : (c + 1) * cols]).astype(BF16)
            for c, p in enumerate(parts)
        ]

    def norm(i, carry):
        rows = pl.ds(pl.multiple_of(i * step, step), step)
        parts = [tokens[rows, c * cols : (c + 1) * cols].astype(F32) for c in range(chunks)]
        for c, part in enumerate(scaled(parts)):
            normed[c, rows, :] = part
        return carry

    lax.fori_loop(0, n_rows // step, norm, 0)
    for copy in local:
        copy.wait()
    for copy in remote:
        copy.wait_recv()
    parts = []
    for h in range(2):
        first = sum(
            jnp.dot(normed[c], sg[h, c * cols : (c + 1) * cols], preferred_element_type=F32)
            for c in range(chunks)
        )
        second = sum(
            jnp.dot(normed[c], su[h, c * cols : (c + 1) * cols], preferred_element_type=F32)
            for c in range(chunks)
        )
        parts.append(silu_mul(first, second).astype(BF16))
    hid = jnp.concatenate(parts, axis=1)
    for c in range(chunks):
        w = sd[:, :, c * cols : (c + 1) * cols].reshape(2 * half, cols)
        total[c] = jnp.dot(hid, w, preferred_element_type=F32)

    def order(i):
        i = lax.rem(i + 1, side)
        return lax.rem(jnp.where(lax.rem(i, 2) == 1, (i + 1) // 2, side - i // 2), side)

    def across(j, c, source_of, target_of, send_sem, recv_sem):
        axis = 1 - first_axis(c)
        mine = at[axis]

        def one(i, carry):
            pos = lax.rem(mine + order(i), side)
            src, dst = source_of(pos), target_of(mine)

            @pl.when(pos == mine)
            def _():
                pltpu.make_async_copy(src, dst, recv_sem.at[c, j]).start()

            @pl.when(pos != mine)
            def _():
                to_peer(axis, pos, src, dst, send_sem.at[c, j], recv_sem.at[c, j])

            return carry

        lax.fori_loop(0, side, one, 0)

    def by_source(ref, j, c, pos):
        return ref.at[c, j, pos] if first_axis(c) == 0 else ref.at[c, j, :, pos]

    for j in range(local_exp):
        for c in range(chunks):
            if relayed:
                wait_for(arrived.at[c, 0, pl.ds(0, relayed)], relay_recv.at[c, j])
            across(
                j,
                c,
                lambda pos: passing.at[c, pos, j],
                lambda mine: by_source(arrived, j, c, mine),
                cross_send,
                cross_recv,
            )

    block = max(1, side // 2)
    for j in range(local_exp):
        for c in range(chunks):
            wait_for(arrived.at[c, 0], cross_recv.at[c, j])

        def norm_rows(i, carry):
            parts = [arrived[c, j, i].reshape(line, cols).astype(F32) for c in range(chunks)]
            for c, part in enumerate(scaled(parts)):
                arrived[c, j, i] = part.reshape(side, cap, cols)
            return carry

        lax.fori_loop(0, side, norm_rows, 0)

        def experts_of(i, carry):
            rows = pl.ds(i * block, block)
            xs = [
                arrived[c, j, rows].reshape(block * line, cols) for c in range(chunks)
            ]
            parts = []
            for h in range(2):
                first = sum(
                    jnp.dot(xs[c], wg[h, j, c * cols : (c + 1) * cols], preferred_element_type=F32)
                    for c in range(chunks)
                )
                second = sum(
                    jnp.dot(xs[c], wu[h, j, c * cols : (c + 1) * cols], preferred_element_type=F32)
                    for c in range(chunks)
                )
                parts.append(silu_mul(first, second).astype(BF16))
            hid = jnp.concatenate(parts, axis=1)
            for c in range(chunks):
                w = wd[:, j, :, c * cols : (c + 1) * cols].reshape(2 * half, cols)
                part = jnp.dot(hid, w, preferred_element_type=F32)
                arrived[c, j, rows] = part.reshape(block, side, cap, cols).astype(BF16)
            return carry

        lax.fori_loop(0, side // block, experts_of, 0)
        for c in range(chunks):
            across(
                j,
                c,
                lambda pos: by_source(arrived, j, c, pos),
                lambda mine: passing_back.at[c, j, :, mine],
                home_send,
                home_recv,
            )

    for j in range(local_exp):
        for c in range(chunks):
            axis = first_axis(c)
            wait_for(arrived.at[c, 0], home_recv.at[c, j])
            for d in range(1, reach):
                for s in range(2):
                    rows = span(d + 2, s)
                    to_peer(
                        axis,
                        ahead(axis, 1 - s, d),
                        passing_back.at[c, j, ahead(axis, 1 - s, d + 2), rows],
                        packed_back.at[c, s, d - 1, j, rows],
                        hub_send.at[c, j],
                        hub_recv.at[c, s],
                    )

    def weigh_own(notes, axis):
        i = lax.broadcasted_iota(jnp.int32, (1, local_exp * line), 1)
        row = (i // line * side + at[axis]) * line + lax.rem(i, line)
        return weigh_rows(notes, row)

    def own_rows(c, pos):
        return [passing_back[c, j, pos].reshape(line, cols) for j in range(local_exp)]

    def product(weights, rows):
        rows = jnp.concatenate(rows, axis=0)
        return sum(jnp.dot(w, rows, preferred_element_type=F32) for w in weights)

    for axis in range(2):
        weights = weigh_own(notes_out[axis], axis)
        for c in range(axis, chunks, 2):
            total[c] += product(weights, own_rows(c, at[axis]))

    for c in range(chunks):
        axis = first_axis(c)
        wait_for(dense.at[c], far_send.at[c])
        for s in range(2):
            i = lax.broadcasted_iota(jnp.int32, (1, reach * local_exp * line), 1)
            d = i // (local_exp * line)
            j_row = lax.rem(i // line, local_exp)
            pos = lax.rem(at[axis] + (d if s == 0 else side - d), side)
            row = (j_row * side + pos) * line + lax.rem(i, line)
            mine = span(side // 2, s)
            second = lax.rem(i, line) // cap
            inside = (second >= mine.start) & (second < mine.start + mine.size)
            row = jnp.where((d < reach - 1) | inside, row, -1)
            weights = weigh_rows(notes_in[axis, s, 1], row)
            rows = own_rows(c, ahead(axis, 1 - s, 2))
            if reach > 1:
                wait_for(
                    arrived.at[c, 0, pl.ds(0, relayed * local_exp // 2)], hub_recv.at[c, s]
                )
                rows += [packed_back[c, s].reshape((reach - 1) * local_exp * line, cols)]
            dense_far[c, s] = product(weights, rows).astype(BF16)
            to_peer(
                axis,
                ahead(axis, 1 - s, 1),
                dense_far.at[c, s],
                chain.at[c, s],
                chain_send.at[c],
                chain_recv.at[c, s],
            )

    for c in range(chunks):
        axis = first_axis(c)
        for s in range(2):
            source = ahead(axis, 1 - s, 1)
            part = product(weigh_own(notes_in[axis, s, 0], axis), own_rows(c, source))
            wait_for(chain.at[c, s], chain_recv.at[c, s])
            dense[c, s] = (part + chain[c, s].astype(F32)).astype(BF16)
            to_peer(
                axis,
                source,
                dense.at[c, s],
                dense_back.at[c, 1 - s],
                sum_send.at[c],
                sum_recv.at[c, 1 - s],
            )

    for c in range(chunks):
        for s in range(2):
            wait_for(dense_back.at[c, s], sum_recv.at[c, s])
        mixed = total[c] + dense_back[c, 0].astype(F32) + dense_back[c, 1].astype(F32)
        out[:, c * cols : (c + 1) * cols] = mixed.astype(BF16)

    for copy in remote:
        copy.wait_send()
    wait_for(notes_in, note_send.at[0])
    for c in range(chunks):
        wait_for(dense.at[c], dense_send.at[c])
        wait_for(dense.at[c], chain_send.at[c])
        wait_for(dense.at[c], sum_send.at[c])
        for j in range(local_exp):
            wait_for(arrived.at[c, 0, pl.ds(0, side - 1)], cross_send.at[c, j])
            wait_for(arrived.at[c, 0, pl.ds(0, side - 1)], home_send.at[c, j])
            if relayed:
                wait_for(arrived.at[c, 0, pl.ds(0, relayed)], relay_send.at[c, j])
                wait_for(arrived.at[c, 0, pl.ds(0, relayed)], hub_send.at[c, j])


def body(n_ep, tokens, norm_gain, expert_ids, gate_values, w_gate, w_up, w_down, s_gate, s_up, s_down):
    n_rows, width = tokens.shape
    topk = expert_ids.shape[1]
    local_exp, _, half = w_gate.shape
    experts = local_exp * n_ep
    cap = 2 * n_rows * topk // experts
    side = math.isqrt(n_ep)
    chunks = 4
    cols = width // chunks
    reach = side // 2 - 1
    vmem = pl.BlockSpec(memory_space=pltpu.VMEM)
    hbm = pl.BlockSpec(memory_space=pl.ANY)
    dma = pltpu.SemaphoreType.DMA

    def tall(*shape):
        return pltpu.VMEM((chunks,) + shape + (cols,), BF16)

    per_expert, per_side = dma((chunks, local_exp)), dma((chunks, 2))
    return pl.pallas_call(
        functools.partial(kernel, n_ep, topk, cap),
        out_shape=jax.ShapeDtypeStruct((n_rows, width), BF16),
        in_specs=[vmem] * 4 + [hbm] * 6,
        out_specs=vmem,
        scratch_shapes=[
            tall(n_rows),
            pltpu.VMEM((2, 8, n_rows), F32),
            pltpu.VMEM((2, 2, 2, 8, n_rows), F32),
            tall(2, n_rows),
            tall(2, n_rows),
            tall(local_exp, 2, max(1, reach - 1), side, cap),
            tall(side, local_exp, side, cap),
            tall(local_exp, side, side, cap),
            tall(local_exp, side, side, cap),
            tall(2, max(1, reach - 1), local_exp, side, cap),
            tall(2, n_rows),
            tall(2, n_rows),
            pltpu.VMEM((chunks, n_rows, cols), F32),
        ]
        + [
            pltpu.VMEM((2,) + w.shape, BF16)
            for w in (w_gate, w_up, w_down, s_gate, s_up, s_down)
        ]
        + [dma((6,))] * 3
        + [dma((1,)), dma((2, 2, 2))]
        + [dma((chunks,)), per_side] * 2
        + [per_expert] * 7
        + [per_side]
        + [dma((chunks,)), per_side] * 2,
        compiler_params=pltpu.CompilerParams(
            collective_id=0, has_side_effects=True, vmem_limit_bytes=VMEM_MIB * 1024 * 1024
        ),
    )(
        tokens,
        norm_gain.reshape(1, width),
        expert_ids.T,
        gate_values.T,
        w_gate,
        w_up,
        w_down,
        s_gate,
        s_up,
        s_down,
    )


def solution(mesh):
    return jax.shard_map(
        functools.partial(body, mesh.shape["ep"]),
        mesh=mesh,
        in_specs=(
            P(("grp", "ep", "tp"), None),
            P(),
            P(("grp", "ep", "tp"), None),
            P(("grp", "ep", "tp"), None),
            P("ep", None, "tp"),
            P("ep", None, "tp"),
            P("ep", "tp", None),
            P(None, "tp"),
            P(None, "tp"),
            P("tp", None),
        ),
        out_specs=P(("grp", "ep", "tp"), None),
        check_vma=False,
    )
```

```python
import functools
import math

import jax
import jax.numpy as jnp
from jax import lax
from jax.experimental import pallas as pl
from jax.experimental.pallas import tpu as pltpu
from jax.sharding import PartitionSpec as P

MESH = pl.DeviceIdType.MESH
BF16, F32 = jnp.bfloat16, jnp.float32
VMEM_MIB = 62


def silu_mul(first, second):
    return first * (1.0 / (1.0 + jnp.exp(-first))) * second


def kernel(
    n_ep,
    topk,
    cap,
    tokens_in,
    gain_in,
    ids_in,
    gates_in,
    w_gate,
    w_up,
    w_down,
    s_gate,
    s_up,
    s_down,
    out,
    tokens,
    gain,
    ids_t,
    gates_t,
    normed,
    notes_out,
    notes_in,
    dense,
    dense_far,
    packed,
    passing,
    arrived,
    passing_back,
    packed_back,
    chain,
    dense_back,
    total,
    wg,
    wu,
    wd,
    sg,
    su,
    sd,
    small_sem,
    token_sem,
    local_sem,
    w_send,
    w_recv,
    note_send,
    note_recv,
    dense_send,
    dense_recv,
    far_send,
    far_recv,
    relay_send,
    relay_recv,
    cross_send,
    cross_recv,
    home_send,
    home_recv,
    hub_send,
    hub_recv,
    chain_send,
    chain_recv,
    sum_send,
    sum_recv,
):
    chunks, n_rows, cols = tokens.shape
    width = chunks * cols
    local_exp = w_gate.shape[0]
    half = w_gate.shape[2]
    experts = local_exp * n_ep
    side = math.isqrt(n_ep)
    line = side * cap
    reach = side // 2 - 1
    relayed = max(0, 2 * reach - 3)
    me = lax.axis_index("ep")
    tp = lax.axis_index("tp")
    at = (lax.rem(me, side), me // side)

    def peer(axis, pos):
        return at[1] * side + pos if axis == 0 else pos * side + at[0]

    def ahead(axis, s, d):
        return lax.rem(at[axis] + (d if s == 0 else side - d), side)

    def first_axis(c):
        return c % 2

    def span(distance, s):
        if distance < side // 2:
            return pl.ds(0, side)
        return pl.ds(s * (side // 2), side // 2)

    barrier = pltpu.get_barrier_semaphore()
    pl.semaphore_signal(barrier, inc=1, device_id={"tp": 1 - tp}, device_id_type=MESH)
    for axis in range(2):

        def greet(i, carry):
            to = peer(axis, lax.rem(at[axis] + i, side))
            pl.semaphore_signal(barrier, inc=1, device_id={"ep": to}, device_id_type=MESH)
            return carry

        lax.fori_loop(1, side, greet, 0)

    pairs = ((s_gate, sg), (s_up, su), (s_down, sd), (w_gate, wg), (w_up, wu), (w_down, wd))
    local = [
        pltpu.make_async_copy(src, dst.at[tp], local_sem.at[i])
        for i, (src, dst) in enumerate(pairs)
    ]
    remote = [
        pltpu.make_async_remote_copy(
            src_ref=src,
            dst_ref=dst.at[tp],
            send_sem=w_send.at[i],
            recv_sem=w_recv.at[i],
            device_id={"tp": 1 - tp},
            device_id_type=MESH,
        )
        for i, (src, dst) in enumerate(pairs)
    ]
    token_loads = [
        pltpu.make_async_copy(
            tokens_in.at[:, c * cols : (c + 1) * cols], tokens.at[c], token_sem.at[c]
        )
        for c in range(chunks)
    ]
    small_loads = [
        pltpu.make_async_copy(src, dst, small_sem.at[i])
        for i, (src, dst) in enumerate(((ids_in, ids_t), (gates_in, gates_t), (gain_in, gain)))
    ]
    for copy in token_loads[:2] + small_loads + token_loads[2:] + local:
        copy.start()

    pl.semaphore_wait(barrier, 2 * side - 1)

    def to_peer(axis, pos, src, dst, send_sem, recv_sem):
        pltpu.make_async_remote_copy(
            src_ref=src,
            dst_ref=dst,
            send_sem=send_sem,
            recv_sem=recv_sem,
            device_id={"ep": peer(axis, pos)},
            device_id_type=MESH,
        ).start()

    def wait_for(part, sem):
        pltpu.make_async_copy(part, part, sem).wait()

    def send_dense(c):
        token_loads[c].wait()
        for s in range(2):
            axis = first_axis(c)
            to_peer(
                axis,
                ahead(axis, s, 1),
                tokens.at[c],
                dense.at[c, s],
                dense_send.at[c],
                dense_recv.at[c, s],
            )

    send_dense(0)
    send_dense(1)

    for copy in small_loads:
        copy.wait()

    expert_of = lax.broadcasted_iota(jnp.int32, (experts, n_rows), 0)
    device_of, j_of = expert_of // local_exp, lax.rem(expert_of, local_exp)
    x_of, y_of = lax.rem(device_of, side), device_of // side
    picks = [ids_t[k : k + 1, :] == expert_of for k in range(topk)]
    used = sum(p.astype(F32) for p in picks).astype(BF16)
    earlier = (
        lax.broadcasted_iota(jnp.int32, (n_rows, n_rows), 0)
        < lax.broadcasted_iota(jnp.int32, (n_rows, n_rows), 1)
    ).astype(F32).astype(BF16)
    slot = jnp.dot(used, earlier, preferred_element_type=F32)
    blank = jnp.zeros((8 - 2 * topk, n_rows), F32)
    for axis in range(2):
        pair = x_of * side + y_of if axis == 0 else y_of * side + x_of
        place = slot + ((j_of * n_ep + pair) * cap).astype(F32)
        notes_out[axis] = jnp.concatenate(
            [jnp.sum(jnp.where(p, place, 0.0), axis=0, keepdims=True) for p in picks]
            + [gates_t[k : k + 1, :] for k in range(topk)]
            + [blank],
            axis=0,
        )
    for axis in range(2):
        for s in range(2):
            for far in range(2):
                to_peer(
                    axis,
                    ahead(axis, s, far + 1),
                    notes_out.at[axis],
                    notes_in.at[axis, s, far],
                    note_send.at[0],
                    note_recv.at[axis, s, far],
                )
    for c in range(2, chunks):
        send_dense(c)
    for copy in remote:
        copy.start()

    def pick_rows(notes, row):
        lanes = [notes[k : k + 1, :].astype(jnp.int32) for k in range(topk)]
        pick = functools.reduce(jnp.logical_or, [row == lane for lane in lanes])
        return pick.astype(F32).astype(BF16)

    def weigh_rows(notes, row):
        by_token = notes.T
        weight = sum(
            jnp.where(
                row == by_token[:, k : k + 1].astype(jnp.int32),
                by_token[:, topk + k : topk + k + 1],
                0.0,
            )
            for k in range(topk)
        )
        high = weight.astype(BF16)
        return high, (weight - high.astype(F32)).astype(BF16)

    def pick_own(notes, axis):
        i = lax.broadcasted_iota(jnp.int32, (local_exp * line, n_rows), 0)
        row = (i // line * side + at[axis]) * line + lax.rem(i, line)
        return pick_rows(notes, row)

    def keep_own(pick, source, pos, c):
        part = jnp.dot(pick, source, preferred_element_type=F32).astype(BF16)
        part = part.reshape(local_exp, side, cap, cols)
        for j in range(local_exp):
            passing[c, :, j, pos] = part[j]

    for axis in range(2):
        pick = pick_own(notes_out[axis], axis)
        for c in range(axis, chunks, 2):
            keep_own(pick, tokens[c], at[axis], c)
    if reach > 1:
        for c in range(chunks):
            for s in range(2):
                for j in range(local_exp):
                    packed_back[c, s, reach - 2, j, span(side // 2, 1 - s)] = jnp.zeros(
                        (side // 2, cap, cols), BF16
                    )

    for c in range(chunks):
        axis = first_axis(c)
        for s in range(2):
            wait_for(dense.at[c, s], dense_recv.at[c, s])
            to_peer(
                axis,
                ahead(axis, s, 1),
                dense.at[c, s],
                dense_far.at[c, s],
                far_send.at[c],
                far_recv.at[c, s],
            )
        for s in range(2):
            if c < 2:
                wait_for(notes_in.at[axis, s, 0], note_recv.at[axis, s, 0])
            pick = pick_own(notes_in[axis, s, 0], axis)
            keep_own(pick, dense[c, s], ahead(axis, 1 - s, 1), c)

    def relay(j, c):
        axis = first_axis(c)
        for s in range(2):
            if j == 0:
                wait_for(dense_far.at[c, s], far_recv.at[c, s])
                if c < 2:
                    wait_for(notes_in.at[axis, s, 1], note_recv.at[axis, s, 1])
            source = ahead(axis, 1 - s, 2)
            i = lax.broadcasted_iota(jnp.int32, (reach * line, n_rows), 0)
            d = i // line
            pos = lax.rem(at[axis] + (d if s == 0 else side - d), side)
            row = (j * side + pos) * line + lax.rem(i, line)
            pick = pick_rows(notes_in[axis, s, 1], row)
            part = jnp.dot(pick, dense_far[c, s], preferred_element_type=F32).astype(BF16)
            part = part.reshape(reach, side, cap, cols)
            if reach > 1:
                packed[c, j, s] = part[1:]
            rows = span(2, s)
            passing[c, rows, j, source] = part[0, rows.start : rows.start + rows.size]
            for d in range(1, reach):
                rows = span(d + 2, s)
                to_peer(
                    axis,
                    ahead(axis, s, d),
                    packed.at[c, j, s, d - 1, rows],
                    passing.at[c, rows, j, source],
                    relay_send.at[c, j],
                    relay_recv.at[c, j],
                )

    for j in range(local_exp):
        for c in range(chunks):
            relay(j, c)

    step = min(32, n_rows)

    def scaled(parts):
        square = sum(jnp.sum(p * p, axis=-1, keepdims=True) for p in parts)
        scale = lax.rsqrt(square * (1.0 / width) + 1e-06)
        return [
            (p * scale * gain[:, c * cols : (c + 1) * cols]).astype(BF16)
            for c, p in enumerate(parts)
        ]

    def norm(i, carry):
        rows = pl.ds(pl.multiple_of(i * step, step), step)
        parts = [tokens[c, rows, :].astype(F32) for c in range(chunks)]
        for c, part in enumerate(scaled(parts)):
            normed[c, rows, :] = part
        return carry

    lax.fori_loop(0, n_rows // step, norm, 0)
    for copy in local:
        copy.wait()
    for copy in remote:
        copy.wait_recv()
    parts = []
    for h in range(2):
        first = sum(
            jnp.dot(normed[c], sg[h, c * cols : (c + 1) * cols], preferred_element_type=F32)
            for c in range(chunks)
        )
        second = sum(
            jnp.dot(normed[c], su[h, c * cols : (c + 1) * cols], preferred_element_type=F32)
            for c in range(chunks)
        )
        parts.append(silu_mul(first, second).astype(BF16))
    hid = jnp.concatenate(parts, axis=1)
    for c in range(chunks):
        w = sd[:, :, c * cols : (c + 1) * cols].reshape(2 * half, cols)
        total[c] = jnp.dot(hid, w, preferred_element_type=F32)

    def order(i):
        i = lax.rem(i + 1, side)
        return lax.rem(jnp.where(lax.rem(i, 2) == 1, (i + 1) // 2, side - i // 2), side)

    def across(j, c, source_of, target_of, send_sem, recv_sem):
        axis = 1 - first_axis(c)
        mine = at[axis]

        def one(i, carry):
            pos = lax.rem(mine + order(i), side)
            src, dst = source_of(pos), target_of(mine)

            @pl.when(pos == mine)
            def _():
                pltpu.make_async_copy(src, dst, recv_sem.at[c, j]).start()

            @pl.when(pos != mine)
            def _():
                to_peer(axis, pos, src, dst, send_sem.at[c, j], recv_sem.at[c, j])

            return carry

        lax.fori_loop(0, side, one, 0)

    def by_source(ref, j, c, pos):
        return ref.at[c, j, pos] if first_axis(c) == 0 else ref.at[c, j, :, pos]

    for j in range(local_exp):
        for c in range(chunks):
            if relayed:
                wait_for(arrived.at[c, 0, pl.ds(0, relayed)], relay_recv.at[c, j])
            across(
                j,
                c,
                lambda pos: passing.at[c, pos, j],
                lambda mine: by_source(arrived, j, c, mine),
                cross_send,
                cross_recv,
            )

    block = max(1, side // 2)
    for j in range(local_exp):
        for c in range(chunks):
            wait_for(arrived.at[c, 0], cross_recv.at[c, j])

        def norm_rows(i, carry):
            parts = [arrived[c, j, i].reshape(line, cols).astype(F32) for c in range(chunks)]
            for c, part in enumerate(scaled(parts)):
                arrived[c, j, i] = part.reshape(side, cap, cols)
            return carry

        lax.fori_loop(0, side, norm_rows, 0)

        def experts_of(i, carry):
            rows = pl.ds(i * block, block)
            xs = [
                arrived[c, j, rows].reshape(block * line, cols) for c in range(chunks)
            ]
            parts = []
            for h in range(2):
                first = sum(
                    jnp.dot(xs[c], wg[h, j, c * cols : (c + 1) * cols], preferred_element_type=F32)
                    for c in range(chunks)
                )
                second = sum(
                    jnp.dot(xs[c], wu[h, j, c * cols : (c + 1) * cols], preferred_element_type=F32)
                    for c in range(chunks)
                )
                parts.append(silu_mul(first, second).astype(BF16))
            hid = jnp.concatenate(parts, axis=1)
            for c in range(chunks):
                w = wd[:, j, :, c * cols : (c + 1) * cols].reshape(2 * half, cols)
                part = jnp.dot(hid, w, preferred_element_type=F32)
                arrived[c, j, rows] = part.reshape(block, side, cap, cols).astype(BF16)
            return carry

        lax.fori_loop(0, side // block, experts_of, 0)
        for c in range(chunks):
            across(
                j,
                c,
                lambda pos: by_source(arrived, j, c, pos),
                lambda mine: passing_back.at[c, j, :, mine],
                home_send,
                home_recv,
            )

    for j in range(local_exp):
        for c in range(chunks):
            axis = first_axis(c)
            wait_for(arrived.at[c, 0], home_recv.at[c, j])
            for d in range(1, reach):
                for s in range(2):
                    rows = span(d + 2, s)
                    to_peer(
                        axis,
                        ahead(axis, 1 - s, d),
                        passing_back.at[c, j, ahead(axis, 1 - s, d + 2), rows],
                        packed_back.at[c, s, d - 1, j, rows],
                        hub_send.at[c, j],
                        hub_recv.at[c, s],
                    )

    def weigh_own(notes, axis):
        i = lax.broadcasted_iota(jnp.int32, (1, local_exp * line), 1)
        row = (i // line * side + at[axis]) * line + lax.rem(i, line)
        return weigh_rows(notes, row)

    def own_rows(c, pos):
        return [passing_back[c, j, pos].reshape(line, cols) for j in range(local_exp)]

    def product(weights, rows):
        rows = jnp.concatenate(rows, axis=0)
        return sum(jnp.dot(w, rows, preferred_element_type=F32) for w in weights)

    for axis in range(2):
        weights = weigh_own(notes_out[axis], axis)
        for c in range(axis, chunks, 2):
            total[c] += product(weights, own_rows(c, at[axis]))

    for c in range(chunks):
        axis = first_axis(c)
        wait_for(dense.at[c], far_send.at[c])
        for s in range(2):
            i = lax.broadcasted_iota(jnp.int32, (1, reach * local_exp * line), 1)
            d = i // (local_exp * line)
            j_row = lax.rem(i // line, local_exp)
            pos = lax.rem(at[axis] + (d if s == 0 else side - d), side)
            row = (j_row * side + pos) * line + lax.rem(i, line)
            mine = span(side // 2, s)
            second = lax.rem(i, line) // cap
            inside = (second >= mine.start) & (second < mine.start + mine.size)
            row = jnp.where((d < reach - 1) | inside, row, -1)
            weights = weigh_rows(notes_in[axis, s, 1], row)
            rows = own_rows(c, ahead(axis, 1 - s, 2))
            if reach > 1:
                wait_for(
                    arrived.at[c, 0, pl.ds(0, relayed * local_exp // 2)], hub_recv.at[c, s]
                )
                rows += [packed_back[c, s].reshape((reach - 1) * local_exp * line, cols)]
            dense_far[c, s] = product(weights, rows).astype(BF16)
            to_peer(
                axis,
                ahead(axis, 1 - s, 1),
                dense_far.at[c, s],
                chain.at[c, s],
                chain_send.at[c],
                chain_recv.at[c, s],
            )

    for c in range(chunks):
        axis = first_axis(c)
        for s in range(2):
            source = ahead(axis, 1 - s, 1)
            part = product(weigh_own(notes_in[axis, s, 0], axis), own_rows(c, source))
            wait_for(chain.at[c, s], chain_recv.at[c, s])
            dense[c, s] = (part + chain[c, s].astype(F32)).astype(BF16)
            to_peer(
                axis,
                source,
                dense.at[c, s],
                dense_back.at[c, 1 - s],
                sum_send.at[c],
                sum_recv.at[c, 1 - s],
            )

    for c in range(chunks):
        for s in range(2):
            wait_for(dense_back.at[c, s], sum_recv.at[c, s])
        mixed = total[c] + dense_back[c, 0].astype(F32) + dense_back[c, 1].astype(F32)
        out[:, c * cols : (c + 1) * cols] = mixed.astype(BF16)

    for copy in remote:
        copy.wait_send()
    wait_for(notes_in, note_send.at[0])
    for c in range(chunks):
        wait_for(dense.at[c], dense_send.at[c])
        wait_for(dense.at[c], chain_send.at[c])
        wait_for(dense.at[c], sum_send.at[c])
        for j in range(local_exp):
            wait_for(arrived.at[c, 0, pl.ds(0, side - 1)], cross_send.at[c, j])
            wait_for(arrived.at[c, 0, pl.ds(0, side - 1)], home_send.at[c, j])
            if relayed:
                wait_for(arrived.at[c, 0, pl.ds(0, relayed)], relay_send.at[c, j])
                wait_for(arrived.at[c, 0, pl.ds(0, relayed)], hub_send.at[c, j])


def body(n_ep, tokens, norm_gain, expert_ids, gate_values, w_gate, w_up, w_down, s_gate, s_up, s_down):
    n_rows, width = tokens.shape
    topk = expert_ids.shape[1]
    local_exp, _, half = w_gate.shape
    experts = local_exp * n_ep
    cap = 2 * n_rows * topk // experts
    side = math.isqrt(n_ep)
    chunks = 4
    cols = width // chunks
    reach = side // 2 - 1
    vmem = pl.BlockSpec(memory_space=pltpu.VMEM)
    hbm = pl.BlockSpec(memory_space=pl.ANY)
    dma = pltpu.SemaphoreType.DMA

    def tall(*shape):
        return pltpu.VMEM((chunks,) + shape + (cols,), BF16)

    per_expert, per_side = dma((chunks, local_exp)), dma((chunks, 2))
    return pl.pallas_call(
        functools.partial(kernel, n_ep, topk, cap),
        out_shape=jax.ShapeDtypeStruct((n_rows, width), BF16),
        in_specs=[hbm] * 10,
        out_specs=vmem,
        scratch_shapes=[
            tall(n_rows),
            pltpu.VMEM((1, width), F32),
            pltpu.VMEM((topk, n_rows), jnp.int32),
            pltpu.VMEM((topk, n_rows), F32),
            tall(n_rows),
            pltpu.VMEM((2, 8, n_rows), F32),
            pltpu.VMEM((2, 2, 2, 8, n_rows), F32),
            tall(2, n_rows),
            tall(2, n_rows),
            tall(local_exp, 2, max(1, reach - 1), side, cap),
            tall(side, local_exp, side, cap),
            tall(local_exp, side, side, cap),
            tall(local_exp, side, side, cap),
            tall(2, max(1, reach - 1), local_exp, side, cap),
            tall(2, n_rows),
            tall(2, n_rows),
            pltpu.VMEM((chunks, n_rows, cols), F32),
        ]
        + [
            pltpu.VMEM((2,) + w.shape, BF16)
            for w in (w_gate, w_up, w_down, s_gate, s_up, s_down)
        ]
        + [dma((3,)), dma((chunks,))]
        + [dma((6,))] * 3
        + [dma((1,)), dma((2, 2, 2))]
        + [dma((chunks,)), per_side] * 2
        + [per_expert] * 7
        + [per_side]
        + [dma((chunks,)), per_side] * 2,
        compiler_params=pltpu.CompilerParams(
            collective_id=0, has_side_effects=True, vmem_limit_bytes=52 * 1024 * 1024
        ),
    )(*[pltpu.with_memory_space_constraint(a, pltpu.HBM) for a in (
        tokens,
        norm_gain.reshape(1, width),
        expert_ids.T,
        gate_values.T,
        w_gate,
        w_up,
        w_down,
        s_gate,
        s_up,
        s_down,
    )])


def solution(mesh):
    return jax.shard_map(
        functools.partial(body, mesh.shape["ep"]),
        mesh=mesh,
        in_specs=(
            P(("grp", "ep", "tp"), None),
            P(),
            P(("grp", "ep", "tp"), None),
            P(("grp", "ep", "tp"), None),
            P("ep", None, "tp"),
            P("ep", None, "tp"),
            P("ep", "tp", None),
            P(None, "tp"),
            P(None, "tp"),
            P("tp", None),
        ),
        out_specs=P(("grp", "ep", "tp"), None),
        check_vma=False,
    )
```

```python
import functools
import math

import jax
import jax.numpy as jnp
from jax import lax
from jax.experimental import pallas as pl
from jax.experimental.pallas import tpu as pltpu
from jax.sharding import PartitionSpec as P

MESH = pl.DeviceIdType.MESH
BF16, F32 = jnp.bfloat16, jnp.float32


def silu_mul(first, second):
    return first * (1.0 / (1.0 + jnp.exp(-first))) * second


def kernel(
    n_ep,
    topk,
    cap,
    tokens_in,
    gain_in,
    ids_in,
    gates_in,
    w_gate,
    w_up,
    w_down,
    s_gate,
    s_up,
    s_down,
    out,
    tokens,
    gain,
    ids_t,
    gates_t,
    normed,
    notes_out,
    notes_in,
    dense,
    dense_far,
    packed,
    passing,
    arrived,
    passing_back,
    packed_back,
    chain,
    dense_back,
    total,
    wg,
    wu,
    wd,
    sg,
    su,
    sd,
    small_sem,
    token_sem,
    local_sem,
    w_send,
    w_recv,
    note_send,
    note_recv,
    dense_send,
    dense_recv,
    far_send,
    far_recv,
    relay_send,
    relay_recv,
    cross_send,
    cross_recv,
    home_send,
    home_recv,
    hub_send,
    hub_recv,
    chain_send,
    chain_recv,
    sum_send,
    sum_recv,
):
    chunks, n_rows, cols = tokens.shape
    width = chunks * cols
    local_exp = w_gate.shape[0]
    half = w_gate.shape[2]
    experts = local_exp * n_ep
    side = math.isqrt(n_ep)
    line = side * cap
    reach = side // 2 - 1
    relayed = max(0, 2 * reach - 3)
    me = lax.axis_index("ep")
    tp = lax.axis_index("tp")
    at = (lax.rem(me, side), me // side)

    def peer(axis, pos):
        return at[1] * side + pos if axis == 0 else pos * side + at[0]

    def ahead(axis, s, d):
        return lax.rem(at[axis] + (d if s == 0 else side - d), side)

    def first_axis(c):
        return c % 2

    def span(distance, s):
        if distance < side // 2:
            return pl.ds(0, side)
        return pl.ds(s * (side // 2), side // 2)

    barrier = pltpu.get_barrier_semaphore()
    pl.semaphore_signal(barrier, inc=1, device_id={"tp": 1 - tp}, device_id_type=MESH)
    for axis in range(2):

        def greet(i, carry):
            to = peer(axis, lax.rem(at[axis] + i, side))
            pl.semaphore_signal(barrier, inc=1, device_id={"ep": to}, device_id_type=MESH)
            return carry

        lax.fori_loop(1, side, greet, 0)

    pairs = ((s_gate, sg), (s_up, su), (s_down, sd), (w_gate, wg), (w_up, wu), (w_down, wd))
    local = [
        pltpu.make_async_copy(src, dst.at[tp], local_sem.at[i])
        for i, (src, dst) in enumerate(pairs)
    ]
    remote = [
        pltpu.make_async_remote_copy(
            src_ref=src,
            dst_ref=dst.at[tp],
            send_sem=w_send.at[i],
            recv_sem=w_recv.at[i],
            device_id={"tp": 1 - tp},
            device_id_type=MESH,
        )
        for i, (src, dst) in enumerate(pairs)
    ]
    token_loads = [
        pltpu.make_async_copy(
            tokens_in.at[:, c * cols : (c + 1) * cols], tokens.at[c], token_sem.at[c]
        )
        for c in range(chunks)
    ]
    small_loads = [
        pltpu.make_async_copy(src, dst, small_sem.at[i])
        for i, (src, dst) in enumerate(((ids_in, ids_t), (gates_in, gates_t), (gain_in, gain)))
    ]
    for copy in token_loads[:2] + small_loads + token_loads[2:] + local:
        copy.start()

    pl.semaphore_wait(barrier, 2 * side - 1)

    def to_peer(axis, pos, src, dst, send_sem, recv_sem):
        pltpu.make_async_remote_copy(
            src_ref=src,
            dst_ref=dst,
            send_sem=send_sem,
            recv_sem=recv_sem,
            device_id={"ep": peer(axis, pos)},
            device_id_type=MESH,
        ).start()

    def wait_for(part, sem):
        pltpu.make_async_copy(part, part, sem).wait()

    def send_dense(c):
        token_loads[c].wait()
        for s in range(2):
            axis = first_axis(c)
            to_peer(
                axis,
                ahead(axis, s, 1),
                tokens.at[c],
                dense.at[c, s],
                dense_send.at[c],
                dense_recv.at[c, s],
            )

    send_dense(0)
    send_dense(1)

    for copy in small_loads:
        copy.wait()

    expert_of = lax.broadcasted_iota(jnp.int32, (experts, n_rows), 0)
    device_of, j_of = expert_of // local_exp, lax.rem(expert_of, local_exp)
    x_of, y_of = lax.rem(device_of, side), device_of // side
    picks = [ids_t[k : k + 1, :] == expert_of for k in range(topk)]
    used = sum(p.astype(F32) for p in picks).astype(BF16)
    earlier = (
        lax.broadcasted_iota(jnp.int32, (n_rows, n_rows), 0)
        < lax.broadcasted_iota(jnp.int32, (n_rows, n_rows), 1)
    ).astype(F32).astype(BF16)
    slot = jnp.dot(used, earlier, preferred_element_type=F32)
    blank = jnp.zeros((8 - 2 * topk, n_rows), F32)
    for axis in range(2):
        pair = x_of * side + y_of if axis == 0 else y_of * side + x_of
        place = slot + ((j_of * n_ep + pair) * cap).astype(F32)
        notes_out[axis] = jnp.concatenate(
            [jnp.sum(jnp.where(p, place, 0.0), axis=0, keepdims=True) for p in picks]
            + [gates_t[k : k + 1, :] for k in range(topk)]
            + [blank],
            axis=0,
        )
    for axis in range(2):
        for s in range(2):
            for far in range(2):
                to_peer(
                    axis,
                    ahead(axis, s, far + 1),
                    notes_out.at[axis],
                    notes_in.at[axis, s, far],
                    note_send.at[0],
                    note_recv.at[axis, s, far],
                )
    for c in range(2, chunks):
        send_dense(c)
    for copy in remote:
        copy.start()

    def pick_rows(notes, row):
        lanes = [notes[k : k + 1, :].astype(jnp.int32) for k in range(topk)]
        pick = functools.reduce(jnp.logical_or, [row == lane for lane in lanes])
        return pick.astype(F32).astype(BF16)

    def weigh_rows(notes, row):
        by_token = notes.T
        weight = sum(
            jnp.where(
                row == by_token[:, k : k + 1].astype(jnp.int32),
                by_token[:, topk + k : topk + k + 1],
                0.0,
            )
            for k in range(topk)
        )
        high = weight.astype(BF16)
        return high, (weight - high.astype(F32)).astype(BF16)

    def pick_own(notes, axis):
        i = lax.broadcasted_iota(jnp.int32, (local_exp * line, n_rows), 0)
        row = (i // line * side + at[axis]) * line + lax.rem(i, line)
        return pick_rows(notes, row)

    def keep_own(pick, source, pos, c):
        part = jnp.dot(pick, source, preferred_element_type=F32).astype(BF16)
        part = part.reshape(local_exp, side, cap, cols)
        for j in range(local_exp):
            passing[c, :, j, pos] = part[j]

    for axis in range(2):
        pick = pick_own(notes_out[axis], axis)
        for c in range(axis, chunks, 2):
            keep_own(pick, tokens[c], at[axis], c)
    if reach > 1:
        for c in range(chunks):
            for s in range(2):
                for j in range(local_exp):
                    packed_back[c, s, reach - 2, j, span(side // 2, 1 - s)] = jnp.zeros(
                        (side // 2, cap, cols), BF16
                    )

    for c in range(chunks):
        axis = first_axis(c)
        for s in range(2):
            wait_for(dense.at[c, s], dense_recv.at[c, s])
            to_peer(
                axis,
                ahead(axis, s, 1),
                dense.at[c, s],
                dense_far.at[c, s],
                far_send.at[c],
                far_recv.at[c, s],
            )
        for s in range(2):
            if c < 2:
                wait_for(notes_in.at[axis, s, 0], note_recv.at[axis, s, 0])
            pick = pick_own(notes_in[axis, s, 0], axis)
            keep_own(pick, dense[c, s], ahead(axis, 1 - s, 1), c)

    def relay(j, c):
        axis = first_axis(c)
        for s in range(2):
            if j == 0:
                wait_for(dense_far.at[c, s], far_recv.at[c, s])
                if c < 2:
                    wait_for(notes_in.at[axis, s, 1], note_recv.at[axis, s, 1])
            source = ahead(axis, 1 - s, 2)
            i = lax.broadcasted_iota(jnp.int32, (reach * line, n_rows), 0)
            d = i // line
            pos = lax.rem(at[axis] + (d if s == 0 else side - d), side)
            row = (j * side + pos) * line + lax.rem(i, line)
            pick = pick_rows(notes_in[axis, s, 1], row)
            part = jnp.dot(pick, dense_far[c, s], preferred_element_type=F32).astype(BF16)
            part = part.reshape(reach, side, cap, cols)
            if reach > 1:
                packed[c, j, s] = part[1:]
            rows = span(2, s)
            passing[c, rows, j, source] = part[0, rows.start : rows.start + rows.size]
            for d in range(1, reach):
                rows = span(d + 2, s)
                to_peer(
                    axis,
                    ahead(axis, s, d),
                    packed.at[c, j, s, d - 1, rows],
                    passing.at[c, rows, j, source],
                    relay_send.at[c, j],
                    relay_recv.at[c, j],
                )

    for j in range(local_exp):
        for c in range(chunks):
            relay(j, c)

    step = min(32, n_rows)

    def scaled(parts):
        square = sum(jnp.sum(p * p, axis=-1, keepdims=True) for p in parts)
        scale = lax.rsqrt(square * (1.0 / width) + 1e-06)
        return [
            (p * scale * gain[:, c * cols : (c + 1) * cols]).astype(BF16)
            for c, p in enumerate(parts)
        ]

    def norm(i, carry):
        rows = pl.ds(pl.multiple_of(i * step, step), step)
        parts = [tokens[c, rows, :].astype(F32) for c in range(chunks)]
        for c, part in enumerate(scaled(parts)):
            normed[c, rows, :] = part
        return carry

    lax.fori_loop(0, n_rows // step, norm, 0)
    for copy in local:
        copy.wait()
    for copy in remote:
        copy.wait_recv()
    parts = []
    for h in range(2):
        first = sum(
            jnp.dot(normed[c], sg[h, c * cols : (c + 1) * cols], preferred_element_type=F32)
            for c in range(chunks)
        )
        second = sum(
            jnp.dot(normed[c], su[h, c * cols : (c + 1) * cols], preferred_element_type=F32)
            for c in range(chunks)
        )
        parts.append(silu_mul(first, second).astype(BF16))
    hid = jnp.concatenate(parts, axis=1)
    for c in range(chunks):
        w = sd[:, :, c * cols : (c + 1) * cols].reshape(2 * half, cols)
        total[c] = jnp.dot(hid, w, preferred_element_type=F32)

    def order(i):
        i = lax.rem(i + 1, side)
        return lax.rem(jnp.where(lax.rem(i, 2) == 1, (i + 1) // 2, side - i // 2), side)

    def across(j, c, source_of, target_of, send_sem, recv_sem):
        axis = 1 - first_axis(c)
        mine = at[axis]

        def one(i, carry):
            pos = lax.rem(mine + order(i), side)
            src, dst = source_of(pos), target_of(mine)

            @pl.when(pos == mine)
            def _():
                pltpu.make_async_copy(src, dst, recv_sem.at[c, j]).start()

            @pl.when(pos != mine)
            def _():
                to_peer(axis, pos, src, dst, send_sem.at[c, j], recv_sem.at[c, j])

            return carry

        lax.fori_loop(0, side, one, 0)

    def by_source(ref, j, c, pos):
        return ref.at[c, j, pos] if first_axis(c) == 0 else ref.at[c, j, :, pos]

    for j in range(local_exp):
        for c in range(chunks):
            if relayed:
                wait_for(arrived.at[c, 0, pl.ds(0, relayed)], relay_recv.at[c, j])
            across(
                j,
                c,
                lambda pos: passing.at[c, pos, j],
                lambda mine: by_source(arrived, j, c, mine),
                cross_send,
                cross_recv,
            )

    block = max(1, side // 2)
    for j in range(local_exp):
        for c in range(chunks):
            wait_for(arrived.at[c, 0], cross_recv.at[c, j])

        def norm_rows(i, carry):
            parts = [arrived[c, j, i].reshape(line, cols).astype(F32) for c in range(chunks)]
            for c, part in enumerate(scaled(parts)):
                arrived[c, j, i] = part.reshape(side, cap, cols)
            return carry

        lax.fori_loop(0, side, norm_rows, 0)

        def experts_of(i, carry):
            rows = pl.ds(i * block, block)
            xs = [
                arrived[c, j, rows].reshape(block * line, cols) for c in range(chunks)
            ]
            parts = []
            for h in range(2):
                first = sum(
                    jnp.dot(xs[c], wg[h, j, c * cols : (c + 1) * cols], preferred_element_type=F32)
                    for c in range(chunks)
                )
                second = sum(
                    jnp.dot(xs[c], wu[h, j, c * cols : (c + 1) * cols], preferred_element_type=F32)
                    for c in range(chunks)
                )
                parts.append(silu_mul(first, second).astype(BF16))
            hid = jnp.concatenate(parts, axis=1)
            for c in range(chunks):
                w = wd[:, j, :, c * cols : (c + 1) * cols].reshape(2 * half, cols)
                part = jnp.dot(hid, w, preferred_element_type=F32)
                arrived[c, j, rows] = part.reshape(block, side, cap, cols).astype(BF16)
            return carry

        lax.fori_loop(0, side // block, experts_of, 0)
        for c in range(chunks):
            across(
                j,
                c,
                lambda pos: by_source(arrived, j, c, pos),
                lambda mine: passing_back.at[c, j, :, mine],
                home_send,
                home_recv,
            )

    far_rows, own_count = reach * local_exp * line, local_exp * line
    for c in range(chunks):
        wait_for(dense.at[c], dense_send.at[c])

    def own_row(axis):
        i = lax.broadcasted_iota(jnp.int32, (1, own_count), 1)
        return (i // line * side + at[axis]) * line + lax.rem(i, line)

    for axis in range(2):
        for s in range(2):
            i = lax.broadcasted_iota(jnp.int32, (1, far_rows), 1)
            d = i // own_count
            j_row = lax.rem(i // line, local_exp)
            pos = lax.rem(at[axis] + (d if s == 0 else side - d), side)
            row = (j_row * side + pos) * line + lax.rem(i, line)
            mine = span(side // 2, s)
            second = lax.rem(i, line) // cap
            inside = (second >= mine.start) & (second < mine.start + mine.size)
            row = jnp.where((d < reach - 1) | inside, row, -1)
            high, low = weigh_rows(notes_in[axis, s, 1], row)
            normed[2 * axis + s, :, :far_rows] = high
            tokens[2 * axis + s, :, :far_rows] = low
            high, low = weigh_rows(notes_in[axis, s, 0], own_row(axis))
            normed[2 * axis + s, :, far_rows : far_rows + own_count] = high
            tokens[2 * axis + s, :, far_rows : far_rows + own_count] = low

    def product(weights, rows):
        rows = jnp.concatenate(rows, axis=0)
        return sum(jnp.dot(w, rows, preferred_element_type=F32) for w in weights)

    def own_rows(c, pos):
        return [passing_back[c, j, pos].reshape(line, cols) for j in range(local_exp)]

    for j in range(local_exp):
        for c in range(chunks):
            axis = first_axis(c)
            wait_for(arrived.at[c, 0], home_recv.at[c, j])
            for d in range(1, reach):
                for s in range(2):
                    rows = span(d + 2, s)
                    to_peer(
                        axis,
                        ahead(axis, 1 - s, d),
                        passing_back.at[c, j, ahead(axis, 1 - s, d + 2), rows],
                        packed_back.at[c, s, d - 1, j, rows],
                        hub_send.at[c, j],
                        hub_recv.at[c, s],
                    )

    for axis in range(2):
        weights = weigh_rows(notes_out[axis], own_row(axis))
        for c in range(axis, chunks, 2):
            total[c] += product(weights, own_rows(c, at[axis]))

    both_axes = [(c + axis, s) for c in range(0, chunks, 2) for s in range(2) for axis in range(2)]

    for c, s in both_axes:
        axis = first_axis(c)
        if s == 0:
            wait_for(dense.at[c], far_send.at[c])
        rows = own_rows(c, ahead(axis, 1 - s, 2))
        if reach > 1:
            wait_for(arrived.at[c, 0, pl.ds(0, relayed * local_exp // 2)], hub_recv.at[c, s])
            rows += [packed_back[c, s].reshape((reach - 1) * own_count, cols)]
        at_gates = 2 * axis + s
        weights = normed[at_gates, :, :far_rows], tokens[at_gates, :, :far_rows]
        dense_far[c, s] = product(weights, rows).astype(BF16)
        to_peer(
            axis,
            ahead(axis, 1 - s, 1),
            dense_far.at[c, s],
            chain.at[c, s],
            chain_send.at[c],
            chain_recv.at[c, s],
        )

    for c, s in both_axes:
        axis = first_axis(c)
        source = ahead(axis, 1 - s, 1)
        own = slice(far_rows, far_rows + own_count)
        weights = normed[2 * axis + s, :, own], tokens[2 * axis + s, :, own]
        part = product(weights, own_rows(c, source))
        wait_for(chain.at[c, s], chain_recv.at[c, s])
        dense[c, s] = (part + chain[c, s].astype(F32)).astype(BF16)
        to_peer(
            axis,
            source,
            dense.at[c, s],
            dense_back.at[c, 1 - s],
            sum_send.at[c],
            sum_recv.at[c, 1 - s],
        )

    for c in range(chunks):
        for s in range(2):
            wait_for(dense_back.at[c, s], sum_recv.at[c, s])
        mixed = total[c] + dense_back[c, 0].astype(F32) + dense_back[c, 1].astype(F32)
        out[:, c * cols : (c + 1) * cols] = mixed.astype(BF16)

    for copy in remote:
        copy.wait_send()
    wait_for(notes_in, note_send.at[0])
    for c in range(chunks):
        wait_for(dense.at[c], chain_send.at[c])
        wait_for(dense.at[c], sum_send.at[c])
        for j in range(local_exp):
            wait_for(arrived.at[c, 0, pl.ds(0, side - 1)], cross_send.at[c, j])
            wait_for(arrived.at[c, 0, pl.ds(0, side - 1)], home_send.at[c, j])
            if relayed:
                wait_for(arrived.at[c, 0, pl.ds(0, relayed)], relay_send.at[c, j])
                wait_for(arrived.at[c, 0, pl.ds(0, relayed)], hub_send.at[c, j])


def body(n_ep, tokens, norm_gain, expert_ids, gate_values, w_gate, w_up, w_down, s_gate, s_up, s_down):
    n_rows, width = tokens.shape
    topk = expert_ids.shape[1]
    local_exp, _, half = w_gate.shape
    experts = local_exp * n_ep
    cap = 2 * n_rows * topk // experts
    side = math.isqrt(n_ep)
    chunks = 4
    cols = width // chunks
    reach = side // 2 - 1
    vmem = pl.BlockSpec(memory_space=pltpu.VMEM)
    hbm = pl.BlockSpec(memory_space=pl.ANY)
    dma = pltpu.SemaphoreType.DMA

    def tall(*shape):
        return pltpu.VMEM((chunks,) + shape + (cols,), BF16)

    per_expert, per_side = dma((chunks, local_exp)), dma((chunks, 2))
    return pl.pallas_call(
        functools.partial(kernel, n_ep, topk, cap),
        out_shape=jax.ShapeDtypeStruct((n_rows, width), BF16),
        in_specs=[hbm] * 10,
        out_specs=vmem,
        scratch_shapes=[
            tall(n_rows),
            pltpu.VMEM((1, width), F32),
            pltpu.VMEM((topk, n_rows), jnp.int32),
            pltpu.VMEM((topk, n_rows), F32),
            tall(n_rows),
            pltpu.VMEM((2, 8, n_rows), F32),
            pltpu.VMEM((2, 2, 2, 8, n_rows), F32),
            tall(2, n_rows),
            tall(2, n_rows),
            tall(local_exp, 2, max(1, reach - 1), side, cap),
            tall(side, local_exp, side, cap),
            tall(local_exp, side, side, cap),
            tall(local_exp, side, side, cap),
            tall(2, max(1, reach - 1), local_exp, side, cap),
            tall(2, n_rows),
            tall(2, n_rows),
            pltpu.VMEM((chunks, n_rows, cols), F32),
        ]
        + [
            pltpu.VMEM((2,) + w.shape, BF16)
            for w in (w_gate, w_up, w_down, s_gate, s_up, s_down)
        ]
        + [dma((3,)), dma((chunks,))]
        + [dma((6,))] * 3
        + [dma((1,)), dma((2, 2, 2))]
        + [dma((chunks,)), per_side] * 2
        + [per_expert] * 7
        + [per_side]
        + [dma((chunks,)), per_side] * 2,
        compiler_params=pltpu.CompilerParams(
            collective_id=0, has_side_effects=True, vmem_limit_bytes=52 * 1024 * 1024
        ),
    )(*[pltpu.with_memory_space_constraint(a, pltpu.HBM) for a in (
        tokens,
        norm_gain.reshape(1, width),
        expert_ids.T,
        gate_values.T,
        w_gate,
        w_up,
        w_down,
        s_gate,
        s_up,
        s_down,
    )])


def solution(mesh):
    return jax.shard_map(
        functools.partial(body, mesh.shape["ep"]),
        mesh=mesh,
        in_specs=(
            P(("grp", "ep", "tp"), None),
            P(),
            P(("grp", "ep", "tp"), None),
            P(("grp", "ep", "tp"), None),
            P("ep", None, "tp"),
            P("ep", None, "tp"),
            P("ep", "tp", None),
            P(None, "tp"),
            P(None, "tp"),
            P("tp", None),
        ),
        out_specs=P(("grp", "ep", "tp"), None),
        check_vma=False,
    )
```

```python
import functools
import math

import jax
import jax.numpy as jnp
from jax import lax
from jax.experimental import pallas as pl
from jax.experimental.pallas import tpu as pltpu
from jax.sharding import PartitionSpec as P

MESH = pl.DeviceIdType.MESH
BF16, F32 = jnp.bfloat16, jnp.float32
VMEM_MIB = 62


def silu_mul(first, second):
    return first * (1.0 / (1.0 + jnp.exp(-first))) * second


def kernel(
    n_ep,
    topk,
    cap,
    tokens_in,
    gain_in,
    ids_in,
    gates_in,
    w_gate,
    w_up,
    w_down,
    s_gate,
    s_up,
    s_down,
    out,
    tokens,
    gain,
    ids_t,
    gates_t,
    normed,
    notes_out,
    notes_in,
    dense,
    dense_far,
    packed,
    passing,
    arrived,
    passing_back,
    packed_back,
    chain,
    dense_back,
    total,
    wg,
    wu,
    wd,
    sg,
    su,
    sd,
    small_sem,
    token_sem,
    local_sem,
    w_send,
    w_recv,
    note_send,
    note_recv,
    dense_send,
    dense_recv,
    far_send,
    far_recv,
    relay_send,
    relay_recv,
    cross_send,
    cross_recv,
    home_send,
    home_recv,
    hub_send,
    hub_recv,
    chain_send,
    chain_recv,
    sum_send,
    sum_recv,
):
    chunks, n_rows, cols = tokens.shape
    width = chunks * cols
    local_exp = w_gate.shape[0]
    half = w_gate.shape[2]
    experts = local_exp * n_ep
    side = math.isqrt(n_ep)
    line = side * cap
    reach = side // 2 - 1
    relayed = max(0, 2 * reach - 3)
    me = lax.axis_index("ep")
    tp = lax.axis_index("tp")
    at = (lax.rem(me, side), me // side)

    def peer(axis, pos):
        return at[1] * side + pos if axis == 0 else pos * side + at[0]

    def ahead(axis, s, d):
        return lax.rem(at[axis] + (d if s == 0 else side - d), side)

    def first_axis(c):
        return c % 2

    def span(distance, s):
        if distance < side // 2:
            return pl.ds(0, side)
        return pl.ds(s * (side // 2), side // 2)

    barrier = pltpu.get_barrier_semaphore()
    pl.semaphore_signal(barrier, inc=1, device_id={"tp": 1 - tp}, device_id_type=MESH)
    near = sorted({1, 2, side - 1, side - 2})
    for step in near:
        for axis in range(2):
            to = peer(axis, lax.rem(at[axis] + step, side))
            pl.semaphore_signal(barrier, inc=1, device_id={"ep": to}, device_id_type=MESH)

    pairs = ((s_gate, sg), (s_up, su), (s_down, sd), (w_gate, wg), (w_up, wu), (w_down, wd))
    local = [
        pltpu.make_async_copy(src, dst.at[tp], local_sem.at[i])
        for i, (src, dst) in enumerate(pairs)
    ]
    remote = [
        pltpu.make_async_remote_copy(
            src_ref=src,
            dst_ref=dst.at[tp],
            send_sem=w_send.at[i],
            recv_sem=w_recv.at[i],
            device_id={"tp": 1 - tp},
            device_id_type=MESH,
        )
        for i, (src, dst) in enumerate(pairs)
    ]
    token_loads = [
        pltpu.make_async_copy(
            tokens_in.at[:, c * cols : (c + 1) * cols], tokens.at[c], token_sem.at[c]
        )
        for c in range(chunks)
    ]
    small_loads = [
        pltpu.make_async_copy(src, dst, small_sem.at[i])
        for i, (src, dst) in enumerate(((ids_in, ids_t), (gates_in, gates_t), (gain_in, gain)))
    ]
    for copy in token_loads[:2] + small_loads + token_loads[2:] + local:
        copy.start()

    pl.semaphore_wait(barrier, 2 * len(near) + 1)

    def to_peer(axis, pos, src, dst, send_sem, recv_sem):
        pltpu.make_async_remote_copy(
            src_ref=src,
            dst_ref=dst,
            send_sem=send_sem,
            recv_sem=recv_sem,
            device_id={"ep": peer(axis, pos)},
            device_id_type=MESH,
        ).start()

    def wait_for(part, sem):
        pltpu.make_async_copy(part, part, sem).wait()

    def send_dense(c):
        token_loads[c].wait()
        for s in range(2):
            axis = first_axis(c)
            to_peer(
                axis,
                ahead(axis, s, 1),
                tokens.at[c],
                dense.at[c, s],
                dense_send.at[c],
                dense_recv.at[c, s],
            )

    send_dense(0)
    send_dense(1)

    for copy in small_loads:
        copy.wait()

    expert_of = lax.broadcasted_iota(jnp.int32, (experts, n_rows), 0)
    device_of, j_of = expert_of // local_exp, lax.rem(expert_of, local_exp)
    x_of, y_of = lax.rem(device_of, side), device_of // side
    picks = [ids_t[k : k + 1, :] == expert_of for k in range(topk)]
    used = sum(p.astype(F32) for p in picks).astype(BF16)
    earlier = (
        lax.broadcasted_iota(jnp.int32, (n_rows, n_rows), 0)
        < lax.broadcasted_iota(jnp.int32, (n_rows, n_rows), 1)
    ).astype(F32).astype(BF16)
    slot = jnp.dot(used, earlier, preferred_element_type=F32)
    blank = jnp.zeros((8 - 2 * topk, n_rows), F32)
    for axis in range(2):
        pair = x_of * side + y_of if axis == 0 else y_of * side + x_of
        place = slot + ((j_of * n_ep + pair) * cap).astype(F32)
        notes_out[axis] = jnp.concatenate(
            [jnp.sum(jnp.where(p, place, 0.0), axis=0, keepdims=True) for p in picks]
            + [gates_t[k : k + 1, :] for k in range(topk)]
            + [blank],
            axis=0,
        )
    for axis in range(2):
        for s in range(2):
            for far in range(2):
                to_peer(
                    axis,
                    ahead(axis, s, far + 1),
                    notes_out.at[axis],
                    notes_in.at[axis, s, far],
                    note_send.at[0],
                    note_recv.at[axis, s, far],
                )
    for c in range(2, chunks):
        send_dense(c)
    for copy in remote:
        copy.start()

    def pick_rows(notes, row):
        lanes = [notes[k : k + 1, :].astype(jnp.int32) for k in range(topk)]
        pick = functools.reduce(jnp.logical_or, [row == lane for lane in lanes])
        return pick.astype(F32).astype(BF16)

    def weigh_rows(notes, row):
        by_token = notes.T
        weight = sum(
            jnp.where(
                row == by_token[:, k : k + 1].astype(jnp.int32),
                by_token[:, topk + k : topk + k + 1],
                0.0,
            )
            for k in range(topk)
        )
        high = weight.astype(BF16)
        return high, (weight - high.astype(F32)).astype(BF16)

    def pick_own(notes, axis):
        i = lax.broadcasted_iota(jnp.int32, (local_exp * line, n_rows), 0)
        row = (i // line * side + at[axis]) * line + lax.rem(i, line)
        return pick_rows(notes, row)

    def keep_own(pick, source, pos, c):
        part = jnp.dot(pick, source, preferred_element_type=F32).astype(BF16)
        part = part.reshape(local_exp, side, cap, cols)
        for j in range(local_exp):
            passing[c, :, j, pos] = part[j]

    for axis in range(2):
        pick = pick_own(notes_out[axis], axis)
        for c in range(axis, chunks, 2):
            keep_own(pick, tokens[c], at[axis], c)
    if reach > 1:
        for c in range(chunks):
            for s in range(2):
                for j in range(local_exp):
                    packed_back[c, s, reach - 2, j, span(side // 2, 1 - s)] = jnp.zeros(
                        (side // 2, cap, cols), BF16
                    )

    for c in range(chunks):
        axis = first_axis(c)
        for s in range(2):
            wait_for(dense.at[c, s], dense_recv.at[c, s])
            to_peer(
                axis,
                ahead(axis, s, 1),
                dense.at[c, s],
                dense_far.at[c, s],
                far_send.at[c],
                far_recv.at[c, s],
            )
        for s in range(2):
            if c < 2:
                wait_for(notes_in.at[axis, s, 0], note_recv.at[axis, s, 0])
            pick = pick_own(notes_in[axis, s, 0], axis)
            keep_own(pick, dense[c, s], ahead(axis, 1 - s, 1), c)

    def relay(j, c):
        axis = first_axis(c)
        for s in range(2):
            if j == 0:
                wait_for(dense_far.at[c, s], far_recv.at[c, s])
                if c < 2:
                    wait_for(notes_in.at[axis, s, 1], note_recv.at[axis, s, 1])
            source = ahead(axis, 1 - s, 2)
            i = lax.broadcasted_iota(jnp.int32, (reach * line, n_rows), 0)
            d = i // line
            pos = lax.rem(at[axis] + (d if s == 0 else side - d), side)
            row = (j * side + pos) * line + lax.rem(i, line)
            pick = pick_rows(notes_in[axis, s, 1], row)
            part = jnp.dot(pick, dense_far[c, s], preferred_element_type=F32).astype(BF16)
            part = part.reshape(reach, side, cap, cols)
            if reach > 1:
                packed[c, j, s] = part[1:]
            rows = span(2, s)
            passing[c, rows, j, source] = part[0, rows.start : rows.start + rows.size]
            for d in range(1, reach):
                rows = span(d + 2, s)
                to_peer(
                    axis,
                    ahead(axis, s, d),
                    packed.at[c, j, s, d - 1, rows],
                    passing.at[c, rows, j, source],
                    relay_send.at[c, j],
                    relay_recv.at[c, j],
                )

    for j in range(local_exp):
        for c in range(chunks):
            relay(j, c)

    step = min(32, n_rows)

    def scaled(parts):
        square = sum(jnp.sum(p * p, axis=-1, keepdims=True) for p in parts)
        scale = lax.rsqrt(square * (1.0 / width) + 1e-06)
        return [
            (p * scale * gain[:, c * cols : (c + 1) * cols]).astype(BF16)
            for c, p in enumerate(parts)
        ]

    def norm(i, carry):
        rows = pl.ds(pl.multiple_of(i * step, step), step)
        parts = [tokens[c, rows, :].astype(F32) for c in range(chunks)]
        for c, part in enumerate(scaled(parts)):
            normed[c, rows, :] = part
        return carry

    lax.fori_loop(0, n_rows // step, norm, 0)
    for copy in local:
        copy.wait()
    for copy in remote:
        copy.wait_recv()
    parts = []
    for h in range(2):
        first = sum(
            jnp.dot(normed[c], sg[h, c * cols : (c + 1) * cols], preferred_element_type=F32)
            for c in range(chunks)
        )
        second = sum(
            jnp.dot(normed[c], su[h, c * cols : (c + 1) * cols], preferred_element_type=F32)
            for c in range(chunks)
        )
        parts.append(silu_mul(first, second).astype(BF16))
    hid = jnp.concatenate(parts, axis=1)
    for c in range(chunks):
        w = sd[:, :, c * cols : (c + 1) * cols].reshape(2 * half, cols)
        total[c] = jnp.dot(hid, w, preferred_element_type=F32)

    def order(i):
        i = lax.rem(i + 1, side)
        return lax.rem(jnp.where(lax.rem(i, 2) == 1, (i + 1) // 2, side - i // 2), side)

    def across(j, c, source_of, target_of, send_sem, recv_sem):
        axis = 1 - first_axis(c)
        mine = at[axis]

        def one(i, carry):
            pos = lax.rem(mine + order(i), side)
            src, dst = source_of(pos), target_of(mine)

            @pl.when(pos == mine)
            def _():
                pltpu.make_async_copy(src, dst, recv_sem.at[c, j]).start()

            @pl.when(pos != mine)
            def _():
                to_peer(axis, pos, src, dst, send_sem.at[c, j], recv_sem.at[c, j])

            return carry

        lax.fori_loop(0, side, one, 0)

    def by_source(ref, j, c, pos):
        return ref.at[c, j, pos] if first_axis(c) == 0 else ref.at[c, j, :, pos]

    for j in range(local_exp):
        for c in range(chunks):
            first = j == 0 and c < 2
            for d in ((0, 1) if first and c == 0 else () if first else (c,)):
                if relayed:
                    wait_for(arrived.at[d, 0, pl.ds(0, relayed)], relay_recv.at[d, j])
            across(
                j,
                c,
                lambda pos: passing.at[c, pos, j],
                lambda mine: by_source(arrived, j, c, mine),
                cross_send,
                cross_recv,
            )

    block = max(1, side // 2)
    for j in range(local_exp):
        for c in range(chunks):
            wait_for(arrived.at[c, 0], cross_recv.at[c, j])

        def norm_rows(i, carry):
            parts = [arrived[c, j, i].reshape(line, cols).astype(F32) for c in range(chunks)]
            for c, part in enumerate(scaled(parts)):
                arrived[c, j, i] = part.reshape(side, cap, cols)
            return carry

        lax.fori_loop(0, side, norm_rows, 0)

        def experts_of(i, carry):
            rows = pl.ds(i * block, block)
            xs = [
                arrived[c, j, rows].reshape(block * line, cols) for c in range(chunks)
            ]
            parts = []
            for h in range(2):
                first = sum(
                    jnp.dot(xs[c], wg[h, j, c * cols : (c + 1) * cols], preferred_element_type=F32)
                    for c in range(chunks)
                )
                second = sum(
                    jnp.dot(xs[c], wu[h, j, c * cols : (c + 1) * cols], preferred_element_type=F32)
                    for c in range(chunks)
                )
                parts.append(silu_mul(first, second).astype(BF16))
            hid = jnp.concatenate(parts, axis=1)
            for c in range(chunks):
                w = wd[:, j, :, c * cols : (c + 1) * cols].reshape(2 * half, cols)
                part = jnp.dot(hid, w, preferred_element_type=F32)
                arrived[c, j, rows] = part.reshape(block, side, cap, cols).astype(BF16)
            return carry

        lax.fori_loop(0, side // block, experts_of, 0)
        for c in range(chunks):
            across(
                j,
                c,
                lambda pos: by_source(arrived, j, c, pos),
                lambda mine: passing_back.at[c, j, :, mine],
                home_send,
                home_recv,
            )

    for j in range(local_exp):
        for c in range(chunks):
            axis = first_axis(c)
            wait_for(arrived.at[c, 0], home_recv.at[c, j])
            for d in range(1, reach):
                for s in range(2):
                    rows = span(d + 2, s)
                    to_peer(
                        axis,
                        ahead(axis, 1 - s, d),
                        passing_back.at[c, j, ahead(axis, 1 - s, d + 2), rows],
                        packed_back.at[c, s, d - 1, j, rows],
                        hub_send.at[c, j],
                        hub_recv.at[c, s],
                    )

    def weigh_own(notes, axis):
        i = lax.broadcasted_iota(jnp.int32, (1, local_exp * line), 1)
        row = (i // line * side + at[axis]) * line + lax.rem(i, line)
        return weigh_rows(notes, row)

    def own_rows(c, pos):
        return [passing_back[c, j, pos].reshape(line, cols) for j in range(local_exp)]

    def product(weights, rows):
        rows = jnp.concatenate(rows, axis=0)
        return sum(jnp.dot(w, rows, preferred_element_type=F32) for w in weights)

    for axis in range(2):
        weights = weigh_own(notes_out[axis], axis)
        for c in range(axis, chunks, 2):
            total[c] += product(weights, own_rows(c, at[axis]))

    for c in range(chunks):
        axis = first_axis(c)
        wait_for(dense.at[c], far_send.at[c])
        for s in range(2):
            i = lax.broadcasted_iota(jnp.int32, (1, reach * local_exp * line), 1)
            d = i // (local_exp * line)
            j_row = lax.rem(i // line, local_exp)
            pos = lax.rem(at[axis] + (d if s == 0 else side - d), side)
            row = (j_row * side + pos) * line + lax.rem(i, line)
            mine = span(side // 2, s)
            second = lax.rem(i, line) // cap
            inside = (second >= mine.start) & (second < mine.start + mine.size)
            row = jnp.where((d < reach - 1) | inside, row, -1)
            weights = weigh_rows(notes_in[axis, s, 1], row)
            rows = own_rows(c, ahead(axis, 1 - s, 2))
            if reach > 1:
                wait_for(
                    arrived.at[c, 0, pl.ds(0, relayed * local_exp // 2)], hub_recv.at[c, s]
                )
                rows += [packed_back[c, s].reshape((reach - 1) * local_exp * line, cols)]
            dense_far[c, s] = product(weights, rows).astype(BF16)
            to_peer(
                axis,
                ahead(axis, 1 - s, 1),
                dense_far.at[c, s],
                chain.at[c, s],
                chain_send.at[c],
                chain_recv.at[c, s],
            )

    for c in range(chunks):
        axis = first_axis(c)
        for s in range(2):
            source = ahead(axis, 1 - s, 1)
            part = product(weigh_own(notes_in[axis, s, 0], axis), own_rows(c, source))
            wait_for(chain.at[c, s], chain_recv.at[c, s])
            dense[c, s] = (part + chain[c, s].astype(F32)).astype(BF16)
            to_peer(
                axis,
                source,
                dense.at[c, s],
                dense_back.at[c, 1 - s],
                sum_send.at[c],
                sum_recv.at[c, 1 - s],
            )

    for c in range(chunks):
        for s in range(2):
            wait_for(dense_back.at[c, s], sum_recv.at[c, s])
        mixed = total[c] + dense_back[c, 0].astype(F32) + dense_back[c, 1].astype(F32)
        out[:, c * cols : (c + 1) * cols] = mixed.astype(BF16)

    for copy in remote:
        copy.wait_send()
    wait_for(notes_in, note_send.at[0])
    for c in range(chunks):
        wait_for(dense.at[c], dense_send.at[c])
        wait_for(dense.at[c], chain_send.at[c])
        wait_for(dense.at[c], sum_send.at[c])
        for j in range(local_exp):
            wait_for(arrived.at[c, 0, pl.ds(0, side - 1)], cross_send.at[c, j])
            wait_for(arrived.at[c, 0, pl.ds(0, side - 1)], home_send.at[c, j])
            if relayed:
                wait_for(arrived.at[c, 0, pl.ds(0, relayed)], relay_send.at[c, j])
                wait_for(arrived.at[c, 0, pl.ds(0, relayed)], hub_send.at[c, j])


def body(n_ep, tokens, norm_gain, expert_ids, gate_values, w_gate, w_up, w_down, s_gate, s_up, s_down):
    n_rows, width = tokens.shape
    topk = expert_ids.shape[1]
    local_exp, _, half = w_gate.shape
    experts = local_exp * n_ep
    cap = 2 * n_rows * topk // experts
    side = math.isqrt(n_ep)
    chunks = 4
    cols = width // chunks
    reach = side // 2 - 1
    vmem = pl.BlockSpec(memory_space=pltpu.VMEM)
    hbm = pl.BlockSpec(memory_space=pl.ANY)
    dma = pltpu.SemaphoreType.DMA

    def tall(*shape):
        return pltpu.VMEM((chunks,) + shape + (cols,), BF16)

    per_expert, per_side = dma((chunks, local_exp)), dma((chunks, 2))
    return pl.pallas_call(
        functools.partial(kernel, n_ep, topk, cap),
        out_shape=jax.ShapeDtypeStruct((n_rows, width), BF16),
        in_specs=[hbm] * 10,
        out_specs=vmem,
        scratch_shapes=[
            tall(n_rows),
            pltpu.VMEM((1, width), F32),
            pltpu.VMEM((topk, n_rows), jnp.int32),
            pltpu.VMEM((topk, n_rows), F32),
            tall(n_rows),
            pltpu.VMEM((2, 8, n_rows), F32),
            pltpu.VMEM((2, 2, 2, 8, n_rows), F32),
            tall(2, n_rows),
            tall(2, n_rows),
            tall(local_exp, 2, max(1, reach - 1), side, cap),
            tall(side, local_exp, side, cap),
            tall(local_exp, side, side, cap),
            tall(local_exp, side, side, cap),
            tall(2, max(1, reach - 1), local_exp, side, cap),
            tall(2, n_rows),
            tall(2, n_rows),
            pltpu.VMEM((chunks, n_rows, cols), F32),
        ]
        + [
            pltpu.VMEM((2,) + w.shape, BF16)
            for w in (w_gate, w_up, w_down, s_gate, s_up, s_down)
        ]
        + [dma((3,)), dma((chunks,))]
        + [dma((6,))] * 3
        + [dma((1,)), dma((2, 2, 2))]
        + [dma((chunks,)), per_side] * 2
        + [per_expert] * 7
        + [per_side]
        + [dma((chunks,)), per_side] * 2,
        compiler_params=pltpu.CompilerParams(
            collective_id=0, has_side_effects=True, vmem_limit_bytes=52 * 1024 * 1024
        ),
    )(*[pltpu.with_memory_space_constraint(a, pltpu.HBM) for a in (
        tokens,
        norm_gain.reshape(1, width),
        expert_ids.T,
        gate_values.T,
        w_gate,
        w_up,
        w_down,
        s_gate,
        s_up,
        s_down,
    )])


def solution(mesh):
    return jax.shard_map(
        functools.partial(body, mesh.shape["ep"]),
        mesh=mesh,
        in_specs=(
            P(("grp", "ep", "tp"), None),
            P(),
            P(("grp", "ep", "tp"), None),
            P(("grp", "ep", "tp"), None),
            P("ep", None, "tp"),
            P("ep", None, "tp"),
            P("ep", "tp", None),
            P(None, "tp"),
            P(None, "tp"),
            P("tp", None),
        ),
        out_specs=P(("grp", "ep", "tp"), None),
        check_vma=False,
    )
```
